256 devices in a mesh: ep: 64 (over z, y, core), tp: 4 (over x).
Axes of the slice: x: 4, y: 4, z: 8, core: 2. Of those that a mesh axis runs over, the one named last changes fastest.
Arguments:
- queries: bfloat16 [16384, 8, 128], P('ep', 'tp'), may hold values from -15 to 15
- keys: bfloat16 [16384, 4, 128], P('ep', 'tp'), may hold values from -6 to 6
- values: bfloat16 [16384, 4, 128], P('ep', 'tp'), may hold values from -6 to 6
- key_bias: bfloat16 [16384, 8], P('ep', 'tp'), may hold values from -20 to 2
- out_weight: bfloat16 [1024, 2048], P('tp'), may hold values from -0.1875 to 0.1875
- tokens_b: bfloat16 [32768, 2048], P(('ep', 'tp')), may hold values from -6 to 6
- moe_gain: bfloat16 [2048], replicated, may hold values from 0.099609375 to 1.8984375
- gate_weight: bfloat16 [64, 2048, 2048], P('ep', None, 'tp'), may hold values from -0.125 to 0.125
- up_weight: bfloat16 [64, 2048, 2048], P('ep', None, 'tp'), may hold values from -0.125 to 0.125
- down_weight: bfloat16 [64, 2048, 2048], P('ep', 'tp'), may hold values from -0.125 to 0.125
- routes: int32 [32768, 2], P(('ep', 'tp')), may hold values from 0 to 63, all different within a row; in each aligned block of 128 rows (0 to 127, 128 to 255, ...) at most 6 rows name the same one
- route_weights: float32 [32768, 2], P(('ep', 'tp')), may hold values from 0.2 to 1
Outputs:
- mixed: bfloat16 [16384, 2048], P(('ep', 'tp'))
- moe_out: bfloat16 [32768, 2048], P(('ep', 'tp'))
The draws below stay inside these ranges and needn't reach their ends.
Inputs may be any that keep to these rules, and one draw needn't show every extreme that they name: `routes`: each row names 2 different experts. In each aligned block of 128 rows (the rows of one device) no expert is named by more than 6 rows, and in some block one expert is named by exactly 6 rows.
All inputs are finite; a program needn't handle non-finite values.
Results may differ from the reference program's by a relative error of at most 0.012.
Values may be sent and summed in bfloat16 or wider, within the bound.
A program may use at most 128 MiB of HBM per device.

```python
import math
import jax
import jax.numpy as jnp
import numpy as np
from jax import lax

D = 2048
HEADS = 8
KV_HEADS = 4
DH = 128
FF = 2048
TOP = 2
TOK_A = 256
TOK_B = 128
EXPERTS = 64
CAP = 6
GROUPS = 4
ATTENTION_TOKENS = 16384
TOKENS_B = 32768


def draw_key_bias(key, part):
    chooser = jax.random.uniform(jax.random.fold_in(key, 11), (HEADS,))
    slow_heads = chooser < 0.5
    slow_level = -jnp.log(ATTENTION_TOKENS * 23.0)
    levels = jnp.where(slow_heads, slow_level, -6.5)
    block_shift = jax.random.uniform(jax.random.fold_in(key, 12), (ATTENTION_TOKENS // TOK_A,), minval=-0.8, maxval=0.8)
    roughness = jax.random.uniform(jax.random.fold_in(key, 13), (ATTENTION_TOKENS, HEADS), minval=-1.0, maxval=1.0)
    release_point = jax.random.randint(jax.random.fold_in(key, 14), (3,), 0, ATTENTION_TOKENS)
    sequence_places = jnp.arange(ATTENTION_TOKENS)
    releasing_now = jnp.any(sequence_places[:, None] == release_point[None, :], axis=1)
    steady = levels[None, :] + jnp.repeat(block_shift, TOK_A)[:, None]
    drawn = jnp.where(releasing_now[:, None], -1.5, steady) + roughness
    return drawn.astype(jnp.float32).astype(jnp.bfloat16)


def shard_levels(rng, extent, split, smallest, largest):
    def one(dim, shards_of):
        draws = jax.random.uniform(jax.random.fold_in(jax.random.fold_in(rng, 6), dim), (shards_of,), jnp.float32, smallest / len(split), largest / len(split))
        return jnp.repeat(jnp.exp(draws), extent[dim] // shards_of).reshape((-1,) + (1,) * (len(extent) - dim - 1))

    factor_of = one(*split[0])
    for cut in split[1:]:
        factor_of = factor_of * one(*cut)
    return factor_of


def deal_out(stream_key, own, number, rows, number_of, top, limit, lean):
    ranking = jax.random.permutation(stream_key, number_of)
    crowded, ordinary = portions_of(number_of, rows * top, limit, lean, True), portions_of(number_of, rows * top, limit, lean, False)
    places = jnp.arange(number_of)

    def named(sizes, turn):
        used = int((sizes > 0).sum())
        fixed = max(1, used // 4)
        shifted = fixed + (places - fixed + turn * (used - fixed)) % max(1, number_of - fixed)
        return jnp.zeros((number_of,), jnp.int32).at[ranking[jnp.where(places < fixed, places, shifted)]].set(jnp.asarray(sizes, jnp.int32))

    sizes = jnp.where(number % 4 == 0, named(crowded, number // 4), named(ordinary, number - number // 4 - 1))
    mixed = jax.random.permutation(jax.random.fold_in(own, 3), number_of)
    donor, receiver = mixed[0:number_of // 2 * 2:2], mixed[1:number_of // 2 * 2:2]
    slack = jnp.minimum(sizes[donor] - 1, limit - sizes[receiver]) // 2
    slack = jnp.where((donor == ranking[0]) | (receiver == ranking[0]) | (sizes[receiver] == 0), 0, jnp.maximum(slack, 0))
    shifted = jax.random.randint(jax.random.fold_in(own, 4), (number_of // 2,), 0, 1 << 20) % (slack + 1)
    sizes = sizes.at[donor].add(-shifted).at[receiver].add(shifted)
    items = jnp.searchsorted(jnp.cumsum(sizes), jnp.arange(rows * top), side="right").astype(jnp.int32)
    table = items.reshape(top, rows).T
    table = table[jax.random.permutation(jax.random.fold_in(own, 1), rows)]
    turn = jax.random.randint(jax.random.fold_in(own, 2), (rows, 1), 0, top)
    return jnp.take_along_axis(table, (jnp.arange(top)[None, :] + turn) % top, axis=1)


def portions_of(count, total, most, skew, full):
    weights = [(1 << 20) // math.isqrt(standing ** skew) + 1 for standing in range(1, count + 1)]
    largest = most if full else min(most, max(-(-total // count), total * weights[0] // sum(weights)))
    least = 1 if total - largest >= count - 1 else 0
    given, spare = [largest] + [least] * (count - 1), total - largest - least * (count - 1)
    while spare > 0:
        candidates = [i for i in range(1, count) if given[i] < largest] or [i for i in range(1, count) if given[i] < most]
        mass, left = sum([weights[i] for i in candidates]), spare
        for i in candidates:
            more = min(most - given[i], max(1, left * weights[i] // mass), spare)
            given[i] = given[i] + more
            spare = spare - more
    return np.array(given)


def bell_draw(own_key, dims, width, bound, split=(), held_as=jnp.bfloat16):
    entries = width * jax.random.normal(own_key, dims, jnp.float32)
    if split:
        entries = entries * shard_levels(own_key, dims, split, -0.22, 0.18)
    return jnp.clip(entries, -bound, bound).astype(held_as)


def setup_inputs(seed: int = 0) -> dict:
    streams_of = jax.random.split(jax.random.key(seed), 13)
    queries = bell_draw(streams_of[0], (ATTENTION_TOKENS, HEADS, DH), 2.5, 15.0, ((0, 64), (1, 4)))
    keys = bell_draw(streams_of[1], (ATTENTION_TOKENS, KV_HEADS, DH), 1.0, 6.0, ((0, 64), (1, 4)))
    values = bell_draw(streams_of[2], (ATTENTION_TOKENS, KV_HEADS, DH), 1.0, 6.0, ((0, 64), (1, 4)))
    key_bias = draw_key_bias(jax.random.fold_in(streams_of[12], 71), 0)
    out_weight = bell_draw(streams_of[4], (HEADS * DH, D), (HEADS * DH) ** -0.5, 0.1875, ((0, 4),))
    tokens_b = bell_draw(streams_of[5], (TOKENS_B, D), 1.0, 6.0, ((0, 256),))
    moe_gain = jnp.clip(1.0 + 0.18 * jax.random.normal(streams_of[6], (D,), jnp.float32), 0.099609375, 1.8984375).astype(jnp.bfloat16)
    gate_weight = bell_draw(streams_of[7], (EXPERTS, D, FF), D ** -0.5, 0.125, ((0, 64), (2, 4)))
    up_weight = bell_draw(streams_of[8], (EXPERTS, D, FF), D ** -0.5, 0.125, ((0, 64), (2, 4)))
    down_weight = bell_draw(streams_of[9], (EXPERTS, FF, D), FF ** -0.5, 0.125, ((0, 64), (1, 4)))
    routes_keys = jax.random.split(jax.random.fold_in(streams_of[10], 1), TOKENS_B // TOK_B)
    routes_turns = jax.random.permutation(jax.random.fold_in(streams_of[10], 3), TOKENS_B // TOK_B)
    routes = jax.vmap(lambda own, number: deal_out(jax.random.fold_in(streams_of[10], 2), own, number, TOK_B, EXPERTS, TOP, CAP, 2))(routes_keys, routes_turns).reshape((TOKENS_B, TOP))
    route_weights = jnp.clip(0.2 + 0.8 * jax.random.uniform(streams_of[11], (TOKENS_B, TOP), jnp.float32) ** shard_levels(streams_of[11], (TOKENS_B, TOP), ((0, 256),), -0.2, 0.2), 0.2, 1.0)
    return dict(queries=queries, keys=keys, values=values, key_bias=key_bias, out_weight=out_weight, tokens_b=tokens_b, moe_gain=moe_gain, gate_weight=gate_weight, up_weight=up_weight, down_weight=down_weight, routes=routes, route_weights=route_weights)


def to_bf_and_back(partial_sum):
    return lax.optimization_barrier(partial_sum.astype(jnp.bfloat16)).astype(jnp.float32)

def stick_rows(query_block, first_pos, keys_all, values_all, bias_all):
    block_len = query_block.shape[0]
    group_size = HEADS // KV_HEADS
    query_f = query_block.astype(jnp.float32).reshape(block_len, KV_HEADS, group_size, DH)
    scores = jnp.einsum('rkgd,skd->kgrs', query_f, keys_all) / math.sqrt(DH)
    scores = scores + bias_all[:, :, None, :]
    query_pos = first_pos + jnp.arange(block_len, dtype=jnp.int32)
    key_pos = jnp.arange(ATTENTION_TOKENS, dtype=jnp.int32)
    earlier = key_pos[None, :] < query_pos[:, None]
    log_keep = jnp.where(earlier, jax.nn.log_sigmoid(-scores), 0.0)
    after = lax.cumsum(log_keep, axis=3, reverse=True) - log_keep
    weights = jnp.where(earlier, jnp.exp(jax.nn.log_sigmoid(scores) + after), 0.0).astype(jnp.bfloat16)
    attended = jnp.einsum('kgrs,skd->rkgd', weights.astype(jnp.float32), values_all)
    return attended.reshape(block_len, HEADS * DH).astype(jnp.bfloat16)

def reference(queries, keys, values, key_bias, out_weight, tokens_b, moe_gain, gate_weight, up_weight, down_weight, routes, route_weights):
    group_size = HEADS // KV_HEADS
    keys_all = keys.astype(jnp.float32)
    values_all = values.astype(jnp.float32)
    bias_all = jnp.transpose(key_bias.astype(jnp.float32).reshape(ATTENTION_TOKENS, KV_HEADS, group_size), (1, 2, 0))
    block_len = math.gcd(ATTENTION_TOKENS, 512)
    block_total = ATTENTION_TOKENS // block_len
    query_blocks = queries.reshape(block_total, block_len, HEADS, DH)
    first_positions = (jnp.arange(block_total) * block_len).astype(jnp.int32)

    def one_block(operands):
        return stick_rows(operands[0], operands[1], keys_all, values_all, bias_all)
    attended = lax.map(one_block, (query_blocks, first_positions)).reshape(ATTENTION_TOKENS, HEADS * DH)
    head_width = HEADS * DH // GROUPS
    mixed_sum = jnp.zeros((ATTENTION_TOKENS, D), jnp.float32)
    for group_no in range(GROUPS):
        lower = group_no * head_width
        partial_sum = jnp.dot(attended[:, lower:lower + head_width], out_weight[lower:lower + head_width], preferred_element_type=jnp.float32)
        mixed_sum = mixed_sum + to_bf_and_back(partial_sum)
    mixed = mixed_sum.astype(jnp.bfloat16)
    tokens_f = tokens_b.astype(jnp.float32)
    normed = (tokens_f * lax.rsqrt(lax.optimization_barrier(jnp.mean(tokens_f * tokens_f, axis=1, keepdims=True)) + 1e-06) * moe_gain.astype(jnp.float32)).astype(jnp.bfloat16)
    block_count = TOKENS_B // TOK_B
    flattened_expert_list = routes.reshape(block_count, TOK_B * TOP)
    onehot = (flattened_expert_list[:, :, None] == jnp.arange(EXPERTS, dtype=jnp.int32)[None, None, :]).astype(jnp.int32)
    earlier_count = jnp.cumsum(onehot, axis=1) - onehot
    slot_index = lax.optimization_barrier(jnp.sum(earlier_count * onehot, axis=2))
    block_ids = jnp.arange(block_count, dtype=jnp.int32)[:, None]
    place = (block_ids * CAP + slot_index).astype(jnp.int32)
    token_ids = (block_ids * TOK_B + jnp.arange(TOK_B * TOP, dtype=jnp.int32)[None, :] // TOP).astype(jnp.int32)
    table_token = jnp.zeros((EXPERTS, block_count * CAP), jnp.int32).at[flattened_expert_list.reshape(-1), place.reshape(-1)].set(token_ids.reshape(-1))
    table_weight = jnp.zeros((EXPERTS, block_count * CAP), jnp.float32).at[flattened_expert_list.reshape(-1), place.reshape(-1)].set(route_weights.astype(jnp.float32).reshape(-1))
    unit_width = FF // GROUPS

    def one_expert(carry, operands):
        gate_e, up_e, down_e, token_list, weight_list = operands
        picked = jnp.take(normed, token_list, axis=0)
        gate_val = jnp.dot(picked, gate_e, preferred_element_type=jnp.float32)
        up_val = jnp.dot(picked, up_e, preferred_element_type=jnp.float32)
        hidden = (jax.nn.silu(gate_val) * up_val).astype(jnp.bfloat16)
        expert_sum = jnp.zeros((token_list.shape[0], D), jnp.float32)
        for group_no in range(GROUPS):
            lower = group_no * unit_width
            partial_sum = jnp.dot(hidden[:, lower:lower + unit_width], down_e[lower:lower + unit_width], preferred_element_type=jnp.float32)
            expert_sum = expert_sum + to_bf_and_back(partial_sum)
        result = to_bf_and_back(expert_sum)
        carry = carry.at[token_list].add(weight_list[:, None] * result)
        return (carry, None)
    moe_total = lax.scan(one_expert, jnp.zeros((TOKENS_B, D), jnp.float32), (gate_weight, up_weight, down_weight, table_token, table_weight))[0]
    moe_out = moe_total.astype(jnp.bfloat16)
    return (mixed, moe_out)
```

```python
import math

import jax
import jax.numpy as jnp
from jax import lax
from jax.experimental import pallas as pl
from jax.experimental.pallas import tpu as pltpu
from jax.sharding import PartitionSpec as P

LOG2E = 1.4426950408889634


def gathered_keys(keys, values, bias, axis):
    rows, kv_heads, head_dim = keys.shape
    kv = jnp.concatenate((keys.reshape(rows, head_dim), values.reshape(rows, head_dim)), axis=1)
    terms = jnp.pad(bias.T, ((0, 16 - bias.shape[1]), (0, 0)))
    return lax.all_gather(jnp.concatenate((kv, terms), axis=0), axis, axis=0, tiled=True)


def mirrored(value, axis):
    count = lax.axis_size(axis)
    return lax.ppermute(value, axis, [(source, count - 1 - source) for source in range(count)])


def split_up(value, dim, length):
    before, after = (value.shape[:dim], value.shape[dim + 1 :])
    return jnp.moveaxis(value.reshape(*before, length, -1, *after), dim, 0)


def summed_on_arrival(value, axis, dim):
    pieces = split_up(value, dim, lax.axis_size(axis))
    arrived = lax.all_to_all(pieces, axis, split_axis=0, concat_axis=0, tiled=True)
    return arrived.astype(jnp.float32).sum(axis=0)


def entry_slots(routes, expert_total):
    flattened_expert_list = routes.reshape(-1)
    onehot = (
        flattened_expert_list[:, None] == jnp.arange(expert_total, dtype=jnp.int32)[None, :]
    ).astype(jnp.int32)
    earlier_count = jnp.cumsum(onehot, axis=0) - onehot
    return (flattened_expert_list, jnp.sum(earlier_count * onehot, axis=1))


def swiglu_rows(piece, gate_cols, up_cols):
    gate_val = jnp.dot(piece, gate_cols, preferred_element_type=jnp.float32)
    up_val = jnp.dot(piece, up_cols, preferred_element_type=jnp.float32)
    return (jax.nn.silu(gate_val) * up_val).astype(jnp.bfloat16)


def attend_kernel(blocks, q_ref, kv_ref, out_ref):
    part = pl.program_id(0)
    heads, half, width = q_ref.shape[1:]
    span = 2 * half
    stride = span + 16
    rows = heads * half
    last = blocks[part]
    q = q_ref[0].reshape(rows, width)
    key_at = lax.broadcasted_iota(jnp.int32, (span, span), 0)
    out_at = lax.broadcasted_iota(jnp.int32, (span, span), 1)
    tri = (key_at >= out_at).astype(jnp.bfloat16)
    scale = LOG2E / math.sqrt(width)

    def scored(block):
        start = pl.multiple_of(block * stride, 16)
        k = kv_ref[pl.ds(start, span), :width]
        raw = lax.dot_general(q, k, (((1,), (1,)), ((), ())), preferred_element_type=jnp.float32)
        terms = kv_ref[pl.ds(start + span, 16), :].astype(jnp.float32) * LOG2E
        bias = jnp.concatenate(
            [jnp.broadcast_to(terms[h : h + 1], (half, span)) for h in range(heads)], axis=0
        )
        return raw * scale + bias

    def summed(scores, earlier):
        soft = jnp.maximum(scores, 0.0) + jnp.log2(1.0 + jnp.exp2(-jnp.abs(scores)))
        if earlier is not None:
            soft = jnp.where(earlier, soft, 0.0)
        high = soft.astype(jnp.bfloat16)
        low = (soft - high.astype(jnp.float32)).astype(jnp.bfloat16)
        return jnp.dot(high, tri, preferred_element_type=jnp.float32) + jnp.dot(
            low, tri, preferred_element_type=jnp.float32
        )

    def added(block, scores, sums, accum, carried, earlier):
        weights = jnp.exp2(scores - sums - carried)
        if earlier is not None:
            weights = jnp.where(earlier, weights, 0.0)
        v = kv_ref[pl.ds(pl.multiple_of(block * stride, 16), span), width:]
        accum = accum + jnp.dot(
            weights.astype(jnp.bfloat16), v, preferred_element_type=jnp.float32
        )
        return accum, carried + sums[:, :1]

    def one(block, state, earlier=None):
        scores = scored(block)
        return added(block, scores, summed(scores, earlier), *state, earlier)

    def two(block, state):
        first, second = scored(block), scored(block - 1)
        first_sums, second_sums = summed(first, None), summed(second, None)
        state = added(block, first, first_sums, *state, None)
        return added(block - 1, second, second_sums, *state, None)

    row_at = lax.broadcasted_iota(jnp.int32, (rows, span), 0) % half + part * half
    earlier = lax.broadcasted_iota(jnp.int32, (rows, span), 1) < row_at
    state = (jnp.zeros((rows, width), jnp.float32), jnp.zeros((rows, 1), jnp.float32))
    state = one(last, state, earlier)
    odd = last % 2
    state = lax.fori_loop(0, odd, lambda i, st: one(last - 1, st), state)
    state = lax.fori_loop(0, last // 2, lambda i, st: two(last - odd - 1 - 2 * i, st), state)
    for h in range(heads):
        out_ref[0, :, h * width : (h + 1) * width] = state[0][h * half : (h + 1) * half].astype(
            jnp.bfloat16
        )


def attend(parts, kv_all, blocks):
    count, heads, half, width = parts.shape
    grid_spec = pltpu.PrefetchScalarGridSpec(
        num_scalar_prefetch=1,
        grid=(count,),
        in_specs=[
            pl.BlockSpec((1, heads, half, width), lambda p, b: (p, 0, 0, 0)),
            pl.BlockSpec(kv_all.shape, lambda p, b: (0, 0), pipeline_mode=pl.Buffered(1)),
        ],
        out_specs=pl.BlockSpec((1, half, heads * width), lambda p, b: (p, 0, 0)),
    )
    pairs = kv_all.shape[0] * heads * half
    return pl.pallas_call(
        attend_kernel,
        grid_spec=grid_spec,
        out_shape=jax.ShapeDtypeStruct((count, half, heads * width), jnp.bfloat16),
        compiler_params=pltpu.CompilerParams(vmem_limit_bytes=40 * 1024 * 1024),
        cost_estimate=pl.CostEstimate(
            flops=pairs * 2048, bytes_accessed=kv_all.size * 2, transcendentals=pairs * 3
        ),
    )(blocks, parts, kv_all)


def body(
    queries,
    keys,
    values,
    key_bias,
    out_weight,
    tokens_b,
    moe_gain,
    gate_weight,
    up_weight,
    down_weight,
    routes,
    route_weights,
):
    tok_rows, local_heads, head_dim = queries.shape
    ep_count = lax.axis_size("ep")
    kv_all = gathered_keys(keys, values, key_bias, "ep")
    device_ep = lax.axis_index("ep")
    half_rows = tok_rows // 2
    by_head = jnp.transpose(queries, (1, 0, 2))
    handed = mirrored(by_head[:, half_rows:], "ep")
    blocks = jnp.stack((device_ep, ep_count - 1 - device_ep)).astype(jnp.int32)
    parts = attend(jnp.stack((by_head[:, :half_rows], handed)), kv_all, blocks)
    attended = jnp.concatenate((parts[0], mirrored(parts[1], "ep")), axis=0)
    tok_b, model_width = tokens_b.shape
    top_count = routes.shape[1]
    expert_total = ep_count * gate_weight.shape[0]
    capacity = max(2, 3 * top_count * tok_b // (2 * expert_total))
    tokens_f = tokens_b.astype(jnp.float32)
    normed = (
        tokens_f
        * lax.rsqrt(jnp.mean(tokens_f * tokens_f, axis=1, keepdims=True) + 1e-06)
        * moe_gain.astype(jnp.float32)
    ).astype(jnp.bfloat16)
    flattened_expert_list, slot_index = entry_slots(routes, expert_total)
    place = flattened_expert_list * capacity + slot_index
    outbound = (
        jnp.zeros((expert_total * capacity, model_width), jnp.bfloat16)
        .at[place]
        .set(jnp.repeat(normed, top_count, axis=0))
    )
    outbound = outbound.reshape(expert_total, capacity, model_width)
    gate_cols = gate_weight[0]
    up_cols = up_weight[0]
    down_rows = down_weight[0]
    arrived = lax.all_to_all(outbound, "ep", split_axis=0, concat_axis=0, tiled=True)
    hidden = swiglu_rows(
        lax.all_gather(arrived.reshape(ep_count * capacity, model_width), "tp", axis=0, tiled=True),
        gate_cols,
        up_cols,
    )
    mixed_sum = summed_on_arrival(
        jnp.dot(attended, out_weight, preferred_element_type=jnp.float32).astype(jnp.bfloat16),
        "tp",
        0,
    ).astype(jnp.bfloat16)
    expert_sum = summed_on_arrival(
        jnp.dot(hidden, down_rows, preferred_element_type=jnp.float32).astype(jnp.bfloat16), "tp", 0
    )
    returned = lax.all_to_all(
        expert_sum.astype(jnp.bfloat16).reshape(ep_count, capacity, model_width),
        "ep",
        split_axis=0,
        concat_axis=0,
        tiled=True,
    )
    picked = jnp.take(returned.reshape(expert_total * capacity, model_width), place, axis=0).astype(
        jnp.float32
    )
    weighted = picked * route_weights.reshape(-1)[:, None]
    moe_out = jnp.sum(weighted.reshape(tok_b, top_count, model_width), axis=1).astype(jnp.bfloat16)
    return (mixed_sum, moe_out)


def solution(mesh):
    in_specs = (
        P("ep", "tp", None),
        P("ep", "tp", None),
        P("ep", "tp", None),
        P("ep", "tp"),
        P("tp", None),
        P(("ep", "tp"), None),
        P(),
        P("ep", None, "tp"),
        P("ep", None, "tp"),
        P("ep", "tp", None),
        P(("ep", "tp"), None),
        P(("ep", "tp"), None),
    )
    out_specs = (P(("ep", "tp"), None), P(("ep", "tp"), None))
    return jax.shard_map(body, mesh=mesh, in_specs=in_specs, out_specs=out_specs, check_vma=False)
```

```python
import math

import jax
import jax.numpy as jnp
from jax import lax
from jax.experimental import pallas as pl
from jax.experimental.pallas import tpu as pltpu
from jax.sharding import PartitionSpec as P

LOG2E = 1.4426950408889634
LANES = 128
SLABS = 8
SLAB = 8
TOP = 2
CAP = 6
HELD = 4


def gathered_keys(keys, values, bias, axis):
    rows, kv_heads, head_dim = keys.shape
    kv = jnp.concatenate((keys.reshape(rows, head_dim), values.reshape(rows, head_dim)), axis=1)
    terms = jnp.pad(bias.T, ((0, 16 - bias.shape[1]), (0, 0)))
    return lax.all_gather(jnp.concatenate((kv, terms), axis=0), axis, axis=0, tiled=True)


def mirrored(value, axis):
    count = lax.axis_size(axis)
    return lax.ppermute(value, axis, [(source, count - 1 - source) for source in range(count)])


def split_up(value, dim, length):
    before, after = (value.shape[:dim], value.shape[dim + 1 :])
    return jnp.moveaxis(value.reshape(*before, length, -1, *after), dim, 0)


def summed_on_arrival(value, axis, dim):
    pieces = split_up(value, dim, lax.axis_size(axis))
    arrived = lax.all_to_all(pieces, axis, split_axis=0, concat_axis=0, tiled=True)
    return arrived.astype(jnp.float32).sum(axis=0)


def round_step(number):
    return ((number + 1) // 2) * (2 * (number % 2) - 1)


def pack_kernel(routes, place, tokens_ref, gain_ref, out_ref, places_ref, rows_ref, counts):
    token_count, width = tokens_ref.shape
    tiles = width // LANES
    out_ref[...] = jnp.zeros_like(out_ref)
    tokens = tokens_ref[...].astype(jnp.float32)
    scale = lax.rsqrt(jnp.mean(tokens * tokens, axis=1, keepdims=True) + 1e-06)
    normed = tokens * scale * gain_ref[...].astype(jnp.float32)
    for tile in range(tiles):
        rows_ref[pl.ds(tile, token_count, stride=tiles), :] = normed[
            :, tile * LANES : (tile + 1) * LANES
        ]

    def cleared(index, carry):
        counts[index] = 0
        return carry

    lax.fori_loop(0, counts.shape[0], cleared, 0)
    slab, spot = place[0], place[1]

    def one(token, carry):
        row = rows_ref[pl.ds(pl.multiple_of(token * tiles, tiles), tiles), :].astype(jnp.bfloat16)
        for choice in range(TOP):
            expert = routes[token * TOP + choice]
            used = counts[expert]
            counts[expert] = used + 1
            away = (expert // SLAB - slab + SLABS) % SLABS
            number = jnp.where(away <= SLABS // 2, jnp.maximum(2 * away - 1, 0), 2 * (SLABS - away))
            side = (expert % SLAB - spot + SLAB) % SLAB
            slot = (number * SLAB + side) * CAP + used
            places_ref[token * TOP + choice] = slot
            out_ref[pl.ds(pl.multiple_of(slot * tiles, tiles), tiles), :] = row
        return carry

    lax.fori_loop(0, token_count, one, 0)


def packed(tokens, gain, routes, place):
    token_count, width = tokens.shape
    tiles = width // LANES
    return pl.pallas_call(
        pack_kernel,
        grid_spec=pltpu.PrefetchScalarGridSpec(
            num_scalar_prefetch=2,
            grid=(1,),
            in_specs=[
                pl.BlockSpec(tokens.shape, lambda i, r, p: (0, 0)),
                pl.BlockSpec((1, width), lambda i, r, p: (0, 0)),
            ],
            out_specs=[
                pl.BlockSpec((SLABS * SLAB * CAP * tiles, LANES), lambda i, r, p: (0, 0)),
                pl.BlockSpec(memory_space=pltpu.SMEM),
            ],
            scratch_shapes=[
                pltpu.VMEM((token_count * tiles, LANES), jnp.float32),
                pltpu.SMEM((SLABS * SLAB,), jnp.int32),
            ],
        ),
        out_shape=[
            jax.ShapeDtypeStruct((SLABS * SLAB * CAP * tiles, LANES), jnp.bfloat16),
            jax.ShapeDtypeStruct((token_count * TOP,), jnp.int32),
        ],
        cost_estimate=pl.CostEstimate(flops=10**7, bytes_accessed=2 * 10**6, transcendentals=128),
        name="pack",
    )(routes.reshape(-1), place, tokens, gain.reshape(1, -1))


def combine_kernel(places, weights, returned_ref, out_ref, rows_ref):
    token_count, width = out_ref.shape
    tiles = width // LANES

    def picked(entry):
        start = pl.multiple_of(places[entry] * tiles, tiles)
        return returned_ref[pl.ds(start, tiles), :].astype(jnp.float32) * weights[entry]

    def one(token, carry):
        rows_ref[pl.ds(pl.multiple_of(token * tiles, tiles), tiles), :] = picked(
            token * TOP
        ) + picked(token * TOP + 1)
        return carry

    lax.fori_loop(0, token_count, one, 0)
    for tile in range(tiles):
        out_ref[:, tile * LANES : (tile + 1) * LANES] = rows_ref[
            pl.ds(tile, token_count, stride=tiles), :
        ].astype(jnp.bfloat16)


def combined(returned, places, weights, width):
    token_count = places.shape[0] // TOP
    tiles = width // LANES
    return pl.pallas_call(
        combine_kernel,
        grid_spec=pltpu.PrefetchScalarGridSpec(
            num_scalar_prefetch=2,
            grid=(1,),
            in_specs=[pl.BlockSpec(returned.shape, lambda i, p, w: (0, 0))],
            out_specs=pl.BlockSpec((token_count, width), lambda i, p, w: (0, 0)),
            scratch_shapes=[pltpu.VMEM((token_count * tiles, LANES), jnp.float32)],
        ),
        out_shape=jax.ShapeDtypeStruct((token_count, width), jnp.bfloat16),
        cost_estimate=pl.CostEstimate(flops=10**7, bytes_accessed=2 * 10**6, transcendentals=0),
        name="combine",
    )(places, weights, returned)


def expert_kernel(
    outbound,
    gate_hbm,
    up_hbm,
    down_hbm,
    out_ref,
    gate,
    up,
    down,
    arrived,
    taken,
    part,
    opp_out,
    near_out,
    far_out,
    opp_in,
    near_in,
    far_in,
    result,
    returned,
    relay,
    weight_sem,
    go_send,
    go_recv,
    take_send,
    take_recv,
    sum_send,
    sum_recv,
    back_send,
    back_recv,
):
    me = lax.axis_index("ep")
    seat = lax.axis_index("tp")
    seats = lax.axis_size("tp")
    slab, spot = me // SLAB, me % SLAB
    width = down.shape[1]
    tiles = width // LANES
    block = CAP * tiles
    group = SLAB * block
    rows = SLAB * CAP

    def target(number, side):
        return ((slab + round_step(number) + SLABS) % SLABS) * SLAB + (spot + side) % SLAB

    def origin(number, side):
        return ((slab - round_step(number) + SLABS) % SLABS) * SLAB + (spot - side + SLAB) % SLAB

    def neighbour(step):
        return (seat + step + seats) % seats

    def piece(ref, number, side):
        return ref.at[pl.ds(pl.multiple_of((number * SLAB + side) * block, block), block)]

    def over_ep(source, landing, number, side, device, send, recv):
        return pltpu.make_async_remote_copy(
            src_ref=piece(source, number, side),
            dst_ref=piece(landing, number, side),
            send_sem=send.at[number],
            recv_sem=recv.at[number],
            device_id={"ep": device},
            device_id_type=pl.DeviceIdType.MESH,
        )

    def over_tp(source, landing, send, recv, step):
        return pltpu.make_async_remote_copy(
            src_ref=source,
            dst_ref=landing,
            send_sem=send,
            recv_sem=recv,
            device_id={"tp": neighbour(step)},
            device_id_type=pl.DeviceIdType.MESH,
        )

    def await_group(ref, sem, number):
        @pl.when(number == 0)
        def _():
            rest = ref.at[pl.ds(block, group - block)]
            pltpu.make_async_copy(rest, rest, sem.at[0]).wait()

        @pl.when(number > 0)
        def _():
            whole = ref.at[pl.ds(pl.multiple_of(number * group, group), group)]
            pltpu.make_async_copy(whole, whole, sem.at[number]).wait()

    def await_one(ref, sem):
        pltpu.make_async_copy(ref, ref, sem).wait()

    loads = [
        pltpu.make_async_copy(source.at[0], landing, weight_sem.at[i])
        for i, (source, landing) in enumerate(((gate_hbm, gate), (up_hbm, up), (down_hbm, down)))
    ]
    for load in loads:
        load.start()

    barrier = pltpu.get_barrier_semaphore()

    def greet(index, carry):
        pl.semaphore_signal(
            barrier,
            inc=1,
            device_id={"ep": target(index // SLAB, index % SLAB)},
            device_id_type=pl.DeviceIdType.MESH,
        )
        return carry

    lax.fori_loop(1, SLABS * SLAB, greet, 0)
    for step in (-1, 1):
        pl.semaphore_signal(
            barrier,
            inc=1,
            device_id={"tp": neighbour(step)},
            device_id_type=pl.DeviceIdType.MESH,
        )
    pl.semaphore_wait(barrier, SLABS * SLAB + 1)

    def dispatch(index, carry):
        number, side = index // SLAB, index % SLAB
        over_ep(
            outbound, arrived, number, side, target(number, side), go_send, go_recv
        ).start()
        return carry

    lax.fori_loop(1, SLABS * SLAB, dispatch, 0)
    arrived[0:block] = outbound[0:block]
    for load in loads:
        load.wait()

    def seat_rows(ref, index, slot):
        return ref.at[index, pl.ds(pl.multiple_of(slot * rows, rows), rows)]

    def take(number):
        await_group(arrived, go_recv, number)
        relay[...] = arrived[pl.ds(pl.multiple_of(number * group, group), group), :].astype(
            jnp.float32
        )
        for tile in range(tiles):
            taken[number, 0:rows, tile * LANES : (tile + 1) * LANES] = relay[
                pl.ds(tile, rows, stride=tiles), :
            ].astype(jnp.bfloat16)
        for slot, step in ((1, 1), (2, -1)):
            over_tp(
                seat_rows(taken, number, 0),
                seat_rows(taken, number, slot),
                take_send.at[number, slot - 1],
                take_recv.at[number, slot],
                step,
            ).start()

    def forward(number):
        odd = number % 2
        slot = 1 + odd
        await_one(seat_rows(taken, number, slot), take_recv.at[number, slot])
        over_tp(
            seat_rows(taken, number, slot),
            seat_rows(taken, number, 3),
            take_send.at[number, 2],
            take_recv.at[number, 3],
            1 - 2 * odd,
        ).start()

    def compute(number):
        odd = number % 2
        far = 1 + odd
        await_one(seat_rows(taken, number, 3 - far), take_recv.at[number, 3 - far])
        await_one(seat_rows(taken, number, 3), take_recv.at[number, 3])
        x = taken[number]
        gated = jnp.dot(x, gate[...], preferred_element_type=jnp.float32)
        raised = jnp.dot(x, up[...], preferred_element_type=jnp.float32)
        hidden = (gated / (1.0 + jnp.exp(-gated)) * raised).astype(jnp.bfloat16)
        held = number % HELD
        for at in range(0, width, 512):
            part[held, :, at : at + 512] = jnp.dot(
                hidden, down[:, at : at + 512], preferred_element_type=jnp.float32
            )
        opp_out[number] = part[held, 3 * rows : 4 * rows].astype(jnp.bfloat16)
        over_tp(
            opp_out.at[number],
            opp_in.at[number],
            sum_send.at[number, 0],
            sum_recv.at[number, 0],
            1 - 2 * odd,
        ).start()
        far_out[number] = seat_rows(part, held, far)[...].astype(jnp.bfloat16)
        over_tp(
            far_out.at[number],
            far_in.at[number],
            sum_send.at[number, 1],
            sum_recv.at[number, 1],
            2 * odd - 1,
        ).start()

    def pass_on(number):
        odd = number % 2
        await_one(opp_in.at[number], sum_recv.at[number, 0])
        near_out[number] = (
            seat_rows(part, number % HELD, 2 - odd)[...] + opp_in[number].astype(jnp.float32)
        ).astype(jnp.bfloat16)
        over_tp(
            near_out.at[number],
            near_in.at[number],
            sum_send.at[number, 2],
            sum_recv.at[number, 2],
            1 - 2 * odd,
        ).start()

    def send_back(number):
        await_one(far_in.at[number], sum_recv.at[number, 1])
        await_one(near_in.at[number], sum_recv.at[number, 2])
        for tile in range(tiles):
            lanes = slice(tile * LANES, (tile + 1) * LANES)
            relay[pl.ds(tile, rows, stride=tiles), :] = (
                part[number % HELD, 0:rows, lanes]
                + far_in[number, :, lanes].astype(jnp.float32)
                + near_in[number, :, lanes].astype(jnp.float32)
            )
        result[pl.ds(pl.multiple_of(number * group, group), group), :] = relay[...].astype(
            jnp.bfloat16
        )

        def give(side, carry):
            over_ep(
                result, returned, number, side, origin(number, side), back_send, back_recv
            ).start()
            return carry

        lax.fori_loop(jnp.where(number == 0, 1, 0), SLAB, give, 0)

    stages = (take, forward, compute, pass_on, send_back)

    def turn(index, carry):
        for late, stage in enumerate(stages):
            number = index - late

            @pl.when(jnp.logical_and(number >= 0, number < SLABS))
            def _(stage=stage, number=number):
                stage(number)

        return carry

    lax.fori_loop(0, SLABS + len(stages) - 1, turn, 0)
    returned[0:block] = result[0:block]

    def finish(number, carry):
        await_group(returned, back_recv, number)
        await_group(outbound, go_send, number)
        await_group(result, back_send, number)
        for index in range(3):
            await_one(opp_out.at[number], take_send.at[number, index])
            await_one(opp_out.at[number], sum_send.at[number, index])
        return carry

    lax.fori_loop(0, SLABS, finish, 0)
    out_ref[...] = returned[...]


def experts(outbound, gate_weight, up_weight, down_weight):
    width, units = gate_weight.shape[1:]
    rows = SLAB * CAP
    tile_rows = outbound.shape[0]
    shares = (SLABS, rows, width)
    flat = pltpu.VMEM((tile_rows, LANES), jnp.bfloat16)
    share = pltpu.VMEM(shares, jnp.bfloat16)
    dma = pltpu.SemaphoreType.DMA
    return pl.pallas_call(
        expert_kernel,
        out_shape=jax.ShapeDtypeStruct(outbound.shape, jnp.bfloat16),
        in_specs=[pl.BlockSpec(memory_space=pltpu.VMEM)]
        + [pl.BlockSpec(memory_space=pl.ANY)] * 3,
        out_specs=pl.BlockSpec(memory_space=pltpu.VMEM),
        scratch_shapes=[
            pltpu.VMEM((width, units), jnp.bfloat16),
            pltpu.VMEM((width, units), jnp.bfloat16),
            pltpu.VMEM((units, width), jnp.bfloat16),
            flat,
            pltpu.VMEM((SLABS, 4 * rows, width), jnp.bfloat16),
            pltpu.VMEM((HELD, 4 * rows, width), jnp.float32),
            share,
            share,
            share,
            share,
            share,
            share,
            flat,
            flat,
            pltpu.VMEM((tile_rows // SLABS, LANES), jnp.float32),
            dma((3,)),
            dma((SLABS,)),
            dma((SLABS,)),
            dma((SLABS, 3)),
            dma((SLABS, 4)),
            dma((SLABS, 3)),
            dma((SLABS, 3)),
            dma((SLABS,)),
            dma((SLABS,)),
        ],
        compiler_params=pltpu.CompilerParams(
            collective_id=0, has_side_effects=True, vmem_limit_bytes=60 * 1024 * 1024
        ),
        cost_estimate=pl.CostEstimate(
            flops=8 * tile_rows * LANES * units * 3, bytes_accessed=10**7, transcendentals=10**6
        ),
        name="experts",
    )(outbound, gate_weight, up_weight, down_weight)


def attend_kernel(blocks, q_ref, kv_ref, out_ref):
    part = pl.program_id(0)
    heads, half, width = q_ref.shape[1:]
    span = 2 * half
    stride = span + 16
    rows = heads * half
    last = blocks[part]
    q = q_ref[0].reshape(rows, width)
    key_at = lax.broadcasted_iota(jnp.int32, (span, span), 0)
    out_at = lax.broadcasted_iota(jnp.int32, (span, span), 1)
    tri = (key_at >= out_at).astype(jnp.bfloat16)
    scale = LOG2E / math.sqrt(width)

    def scored(block):
        start = pl.multiple_of(block * stride, 16)
        k = kv_ref[pl.ds(start, span), :width]
        raw = lax.dot_general(q, k, (((1,), (1,)), ((), ())), preferred_element_type=jnp.float32)
        terms = kv_ref[pl.ds(start + span, 16), :].astype(jnp.float32) * LOG2E
        bias = jnp.concatenate(
            [jnp.broadcast_to(terms[h : h + 1], (half, span)) for h in range(heads)], axis=0
        )
        return raw * scale + bias

    def summed(scores, earlier):
        soft = jnp.maximum(scores, 0.0) + jnp.log2(1.0 + jnp.exp2(-jnp.abs(scores)))
        if earlier is not None:
            soft = jnp.where(earlier, soft, 0.0)
        high = soft.astype(jnp.bfloat16)
        low = (soft - high.astype(jnp.float32)).astype(jnp.bfloat16)
        return jnp.dot(high, tri, preferred_element_type=jnp.float32) + jnp.dot(
            low, tri, preferred_element_type=jnp.float32
        )

    def added(block, scores, sums, accum, carried, earlier):
        weights = jnp.exp2(scores - sums - carried)
        if earlier is not None:
            weights = jnp.where(earlier, weights, 0.0)
        v = kv_ref[pl.ds(pl.multiple_of(block * stride, 16), span), width:]
        accum = accum + jnp.dot(
            weights.astype(jnp.bfloat16), v, preferred_element_type=jnp.float32
        )
        return accum, carried + sums[:, :1]

    def one(block, state, earlier=None):
        scores = scored(block)
        return added(block, scores, summed(scores, earlier), *state, earlier)

    def two(block, state):
        first, second = scored(block), scored(block - 1)
        first_sums, second_sums = summed(first, None), summed(second, None)
        state = added(block, first, first_sums, *state, None)
        return added(block - 1, second, second_sums, *state, None)

    row_at = lax.broadcasted_iota(jnp.int32, (rows, span), 0) % half + part * half
    earlier = lax.broadcasted_iota(jnp.int32, (rows, span), 1) < row_at
    state = (jnp.zeros((rows, width), jnp.float32), jnp.zeros((rows, 1), jnp.float32))
    state = one(last, state, earlier)
    odd = last % 2
    state = lax.fori_loop(0, odd, lambda i, st: one(last - 1, st), state)
    state = lax.fori_loop(0, last // 2, lambda i, st: two(last - odd - 1 - 2 * i, st), state)
    for h in range(heads):
        out_ref[0, :, h * width : (h + 1) * width] = state[0][h * half : (h + 1) * half].astype(
            jnp.bfloat16
        )


def attend(parts, kv_all, blocks):
    count, heads, half, width = parts.shape
    grid_spec = pltpu.PrefetchScalarGridSpec(
        num_scalar_prefetch=1,
        grid=(count,),
        in_specs=[
            pl.BlockSpec((1, heads, half, width), lambda p, b: (p, 0, 0, 0)),
            pl.BlockSpec(kv_all.shape, lambda p, b: (0, 0), pipeline_mode=pl.Buffered(1)),
        ],
        out_specs=pl.BlockSpec((1, half, heads * width), lambda p, b: (p, 0, 0)),
    )
    pairs = kv_all.shape[0] * heads * half
    return pl.pallas_call(
        attend_kernel,
        grid_spec=grid_spec,
        out_shape=jax.ShapeDtypeStruct((count, half, heads * width), jnp.bfloat16),
        compiler_params=pltpu.CompilerParams(vmem_limit_bytes=40 * 1024 * 1024),
        cost_estimate=pl.CostEstimate(
            flops=pairs * 2048, bytes_accessed=kv_all.size * 2, transcendentals=pairs * 3
        ),
    )(blocks, parts, kv_all)


def body(
    queries,
    keys,
    values,
    key_bias,
    out_weight,
    tokens_b,
    moe_gain,
    gate_weight,
    up_weight,
    down_weight,
    routes,
    route_weights,
):
    tok_rows, local_heads, head_dim = queries.shape
    ep_count = lax.axis_size("ep")
    kv_all = gathered_keys(keys, values, key_bias, "ep")
    device_ep = lax.axis_index("ep")
    half_rows = tok_rows // 2
    by_head = jnp.transpose(queries, (1, 0, 2))
    handed = mirrored(by_head[:, half_rows:], "ep")
    place = jnp.stack((device_ep // SLAB, device_ep % SLAB)).astype(jnp.int32)
    outbound, places = packed(tokens_b, moe_gain, routes, place)
    returned = experts(outbound, gate_weight, up_weight, down_weight)
    halves = jnp.stack((by_head[:, :half_rows], handed))
    halves, returned = lax.optimization_barrier((halves, returned))
    blocks = jnp.stack((device_ep, ep_count - 1 - device_ep)).astype(jnp.int32)
    parts = attend(halves, kv_all, blocks)
    attended = jnp.concatenate((parts[0], mirrored(parts[1], "ep")), axis=0)
    moe_out = combined(returned, places, route_weights.reshape(-1), tokens_b.shape[1])
    mixed_sum = summed_on_arrival(
        jnp.dot(attended, out_weight, preferred_element_type=jnp.float32).astype(jnp.bfloat16),
        "tp",
        0,
    ).astype(jnp.bfloat16)
    return (mixed_sum, moe_out)


def solution(mesh):
    in_specs = (
        P("ep", "tp", None),
        P("ep", "tp", None),
        P("ep", "tp", None),
        P("ep", "tp"),
        P("tp", None),
        P(("ep", "tp"), None),
        P(),
        P("ep", None, "tp"),
        P("ep", None, "tp"),
        P("ep", "tp", None),
        P(("ep", "tp"), None),
        P(("ep", "tp"), None),
    )
    out_specs = (P(("ep", "tp"), None), P(("ep", "tp"), None))
    return jax.shard_map(body, mesh=mesh, in_specs=in_specs, out_specs=out_specs, check_vma=False)
```

```python
import math

import jax
import jax.numpy as jnp
from jax import lax
from jax.experimental import pallas as pl
from jax.experimental.pallas import tpu as pltpu
from jax.sharding import PartitionSpec as P

LOG2E = 1.4426950408889634
LANES = 128
SLABS = 8
SLAB = 8
TOP = 2
CAP = 6
HELD = 4
STEPS = (0, 2, -2, 4, 3, -3, 1, -1)


def gathered_keys(keys, values, bias, axis):
    rows, kv_heads, head_dim = keys.shape
    kv = jnp.concatenate((keys.reshape(rows, head_dim), values.reshape(rows, head_dim)), axis=1)
    terms = jnp.pad(bias.T, ((0, 16 - bias.shape[1]), (0, 0)))
    return lax.all_gather(jnp.concatenate((kv, terms), axis=0), axis, axis=0, tiled=True)


def mirrored(value, axis):
    count = lax.axis_size(axis)
    return lax.ppermute(value, axis, [(source, count - 1 - source) for source in range(count)])


def split_up(value, dim, length):
    before, after = (value.shape[:dim], value.shape[dim + 1 :])
    return jnp.moveaxis(value.reshape(*before, length, -1, *after), dim, 0)


def summed_on_arrival(value, axis, dim):
    pieces = split_up(value, dim, lax.axis_size(axis))
    arrived = lax.all_to_all(pieces, axis, split_axis=0, concat_axis=0, tiled=True)
    return arrived.astype(jnp.float32).sum(axis=0)


def round_step(number):
    step = 0
    for at, value in enumerate(STEPS):
        step = jnp.where(number == at, value, step)
    return step


def pack_kernel(routes, place, tokens_ref, gain_ref, out_ref, places_ref, rows_ref, counts):
    token_count, width = tokens_ref.shape
    tiles = width // LANES
    out_ref[...] = jnp.zeros_like(out_ref)
    tokens = tokens_ref[...].astype(jnp.float32)
    scale = lax.rsqrt(jnp.mean(tokens * tokens, axis=1, keepdims=True) + 1e-06)
    normed = tokens * scale * gain_ref[...].astype(jnp.float32)
    for tile in range(tiles):
        rows_ref[pl.ds(tile, token_count, stride=tiles), :] = normed[
            :, tile * LANES : (tile + 1) * LANES
        ]

    slab, spot = place[0], place[1]

    def opened(index, carry):
        number, side = index // SLAB, index % SLAB
        home = ((slab + round_step(number) + SLABS) % SLABS) * SLAB + (spot + side) % SLAB
        counts[home] = index * CAP
        return carry

    lax.fori_loop(0, counts.shape[0], opened, 0)

    def one(token, carry):
        row = rows_ref[pl.ds(pl.multiple_of(token * tiles, tiles), tiles), :].astype(jnp.bfloat16)
        for choice in range(TOP):
            expert = routes[token * TOP + choice]
            slot = counts[expert]
            counts[expert] = slot + 1
            places_ref[token * TOP + choice] = slot
            out_ref[pl.ds(pl.multiple_of(slot * tiles, tiles), tiles), :] = row
        return carry

    lax.fori_loop(0, token_count, one, 0, unroll=4)


def packed(tokens, gain, routes, place):
    token_count, width = tokens.shape
    tiles = width // LANES
    return pl.pallas_call(
        pack_kernel,
        grid_spec=pltpu.PrefetchScalarGridSpec(
            num_scalar_prefetch=2,
            grid=(1,),
            in_specs=[
                pl.BlockSpec(tokens.shape, lambda i, r, p: (0, 0)),
                pl.BlockSpec((1, width), lambda i, r, p: (0, 0)),
            ],
            out_specs=[
                pl.BlockSpec((SLABS * SLAB * CAP * tiles, LANES), lambda i, r, p: (0, 0)),
                pl.BlockSpec(memory_space=pltpu.SMEM),
            ],
            scratch_shapes=[
                pltpu.VMEM((token_count * tiles, LANES), jnp.float32),
                pltpu.SMEM((SLABS * SLAB,), jnp.int32),
            ],
        ),
        out_shape=[
            jax.ShapeDtypeStruct((SLABS * SLAB * CAP * tiles, LANES), jnp.bfloat16),
            jax.ShapeDtypeStruct((token_count * TOP,), jnp.int32),
        ],
        cost_estimate=pl.CostEstimate(flops=10**7, bytes_accessed=2 * 10**6, transcendentals=128),
        name="pack",
    )(routes.reshape(-1), place, tokens, gain.reshape(1, -1))


def combine_kernel(places, weights, returned_ref, out_ref, rows_ref):
    token_count, width = out_ref.shape
    tiles = width // LANES

    def picked(entry):
        start = pl.multiple_of(places[entry] * tiles, tiles)
        return returned_ref[pl.ds(start, tiles), :].astype(jnp.float32) * weights[entry]

    def one(token, carry):
        rows_ref[pl.ds(pl.multiple_of(token * tiles, tiles), tiles), :] = picked(
            token * TOP
        ) + picked(token * TOP + 1)
        return carry

    lax.fori_loop(0, token_count, one, 0, unroll=4)
    for tile in range(tiles):
        out_ref[:, tile * LANES : (tile + 1) * LANES] = rows_ref[
            pl.ds(tile, token_count, stride=tiles), :
        ].astype(jnp.bfloat16)


def combined(returned, places, weights, width):
    token_count = places.shape[0] // TOP
    tiles = width // LANES
    return pl.pallas_call(
        combine_kernel,
        grid_spec=pltpu.PrefetchScalarGridSpec(
            num_scalar_prefetch=2,
            grid=(1,),
            in_specs=[pl.BlockSpec(returned.shape, lambda i, p, w: (0, 0))],
            out_specs=pl.BlockSpec((token_count, width), lambda i, p, w: (0, 0)),
            scratch_shapes=[pltpu.VMEM((token_count * tiles, LANES), jnp.float32)],
        ),
        out_shape=jax.ShapeDtypeStruct((token_count, width), jnp.bfloat16),
        cost_estimate=pl.CostEstimate(flops=10**7, bytes_accessed=2 * 10**6, transcendentals=0),
        name="combine",
    )(places, weights, returned)


def expert_kernel(
    outbound,
    gate_hbm,
    up_hbm,
    down_hbm,
    out_ref,
    gate,
    up,
    down,
    arrived,
    taken,
    part,
    opp_out,
    near_out,
    far_out,
    opp_in,
    near_in,
    far_in,
    result,
    returned,
    relay,
    weight_sem,
    go_send,
    go_recv,
    take_send,
    take_recv,
    sum_send,
    sum_recv,
    back_send,
    back_recv,
):
    me = lax.axis_index("ep")
    seat = lax.axis_index("tp")
    seats = lax.axis_size("tp")
    slab, spot = me // SLAB, me % SLAB
    width = down.shape[1]
    tiles = width // LANES
    block = CAP * tiles
    group = SLAB * block
    rows = SLAB * CAP

    def target(number, side):
        return ((slab + round_step(number) + SLABS) % SLABS) * SLAB + (spot + side) % SLAB

    def origin(number, side):
        return ((slab - round_step(number) + SLABS) % SLABS) * SLAB + (spot - side + SLAB) % SLAB

    def neighbour(step):
        return (seat + step + seats) % seats

    def piece(ref, number, side):
        return ref.at[pl.ds(pl.multiple_of((number * SLAB + side) * block, block), block)]

    def over_ep(source, landing, number, side, device, send, recv):
        return pltpu.make_async_remote_copy(
            src_ref=piece(source, number, side),
            dst_ref=piece(landing, number, side),
            send_sem=send.at[number],
            recv_sem=recv.at[number],
            device_id={"ep": device},
            device_id_type=pl.DeviceIdType.MESH,
        )

    def over_tp(source, landing, send, recv, step):
        return pltpu.make_async_remote_copy(
            src_ref=source,
            dst_ref=landing,
            send_sem=send,
            recv_sem=recv,
            device_id={"tp": neighbour(step)},
            device_id_type=pl.DeviceIdType.MESH,
        )

    def await_group(ref, sem, number):
        @pl.when(number == 0)
        def _():
            rest = ref.at[pl.ds(block, group - block)]
            pltpu.make_async_copy(rest, rest, sem.at[0]).wait()

        @pl.when(number > 0)
        def _():
            whole = ref.at[pl.ds(pl.multiple_of(number * group, group), group)]
            pltpu.make_async_copy(whole, whole, sem.at[number]).wait()

    def await_one(ref, sem):
        pltpu.make_async_copy(ref, ref, sem).wait()

    loads = [
        pltpu.make_async_copy(source.at[0], landing, weight_sem.at[i])
        for i, (source, landing) in enumerate(((gate_hbm, gate), (up_hbm, up), (down_hbm, down)))
    ]
    for load in loads:
        load.start()

    barrier = pltpu.get_barrier_semaphore()

    def greet(index, carry):
        pl.semaphore_signal(
            barrier,
            inc=1,
            device_id={"ep": target(index // SLAB, index % SLAB)},
            device_id_type=pl.DeviceIdType.MESH,
        )
        return carry

    lax.fori_loop(1, SLABS * SLAB, greet, 0)
    for step in (-1, 1):
        pl.semaphore_signal(
            barrier,
            inc=1,
            device_id={"tp": neighbour(step)},
            device_id_type=pl.DeviceIdType.MESH,
        )
    pl.semaphore_wait(barrier, SLABS * SLAB + 1)

    def dispatch(index, carry):
        number, side = index // SLAB, index % SLAB
        over_ep(
            outbound, arrived, number, side, target(number, side), go_send, go_recv
        ).start()
        return carry

    lax.fori_loop(1, SLABS * SLAB, dispatch, 0)
    arrived[0:block] = outbound[0:block]
    for load in loads:
        load.wait()

    def seat_rows(ref, index, slot):
        return ref.at[index, pl.ds(pl.multiple_of(slot * rows, rows), rows)]

    def take(number):
        await_group(arrived, go_recv, number)
        relay[...] = arrived[pl.ds(pl.multiple_of(number * group, group), group), :].astype(
            jnp.float32
        )
        for tile in range(tiles):
            taken[number, 0:rows, tile * LANES : (tile + 1) * LANES] = relay[
                pl.ds(tile, rows, stride=tiles), :
            ].astype(jnp.bfloat16)
        for slot, step in ((1, 1), (2, -1)):
            over_tp(
                seat_rows(taken, number, 0),
                seat_rows(taken, number, slot),
                take_send.at[number, slot - 1],
                take_recv.at[number, slot],
                step,
            ).start()

    def forward(number):
        odd = number % 2
        slot = 1 + odd
        await_one(seat_rows(taken, number, slot), take_recv.at[number, slot])
        over_tp(
            seat_rows(taken, number, slot),
            seat_rows(taken, number, 3),
            take_send.at[number, 2],
            take_recv.at[number, 3],
            1 - 2 * odd,
        ).start()

    def compute(number):
        odd = number % 2
        far = 1 + odd
        await_one(seat_rows(taken, number, 3 - far), take_recv.at[number, 3 - far])
        await_one(seat_rows(taken, number, 3), take_recv.at[number, 3])
        x = taken[number]
        gated = jnp.dot(x, gate[...], preferred_element_type=jnp.float32)
        raised = jnp.dot(x, up[...], preferred_element_type=jnp.float32)
        hidden = (gated / (1.0 + jnp.exp(-gated)) * raised).astype(jnp.bfloat16)
        held = number % HELD
        for at in range(0, width, 512):
            part[held, :, at : at + 512] = jnp.dot(
                hidden, down[:, at : at + 512], preferred_element_type=jnp.float32
            )
        opp_out[number] = part[held, 3 * rows : 4 * rows].astype(jnp.bfloat16)
        over_tp(
            opp_out.at[number],
            opp_in.at[number],
            sum_send.at[number, 0],
            sum_recv.at[number, 0],
            2 * odd - 1,
        ).start()
        far_out[number] = seat_rows(part, held, 2 - odd)[...].astype(jnp.bfloat16)
        over_tp(
            far_out.at[number],
            far_in.at[number],
            sum_send.at[number, 1],
            sum_recv.at[number, 1],
            1 - 2 * odd,
        ).start()

    def pass_on(number):
        odd = number % 2
        await_one(opp_in.at[number], sum_recv.at[number, 0])
        near_out[number] = (
            seat_rows(part, number % HELD, 1 + odd)[...] + opp_in[number].astype(jnp.float32)
        ).astype(jnp.bfloat16)
        over_tp(
            near_out.at[number],
            near_in.at[number],
            sum_send.at[number, 2],
            sum_recv.at[number, 2],
            2 * odd - 1,
        ).start()

    def send_back(number):
        await_one(far_in.at[number], sum_recv.at[number, 1])
        await_one(near_in.at[number], sum_recv.at[number, 2])
        for tile in range(tiles):
            lanes = slice(tile * LANES, (tile + 1) * LANES)
            relay[pl.ds(tile, rows, stride=tiles), :] = (
                part[number % HELD, 0:rows, lanes]
                + far_in[number, :, lanes].astype(jnp.float32)
                + near_in[number, :, lanes].astype(jnp.float32)
            )
        result[pl.ds(pl.multiple_of(number * group, group), group), :] = relay[...].astype(
            jnp.bfloat16
        )

        def give(side, carry):
            over_ep(
                result, returned, number, side, origin(number, side), back_send, back_recv
            ).start()
            return carry

        lax.fori_loop(jnp.where(number == 0, 1, 0), SLAB, give, 0)

    stages = (take, forward, compute, pass_on, send_back)

    def turn(index, carry):
        for late, stage in enumerate(stages):
            number = index - late

            @pl.when(jnp.logical_and(number >= 0, number < SLABS))
            def _(stage=stage, number=number):
                stage(number)

        return carry

    lax.fori_loop(0, SLABS + len(stages) - 1, turn, 0)
    returned[0:block] = result[0:block]

    def finish(number, carry):
        await_group(returned, back_recv, number)
        await_group(outbound, go_send, number)
        await_group(result, back_send, number)
        for index in range(3):
            await_one(opp_out.at[number], take_send.at[number, index])
            await_one(opp_out.at[number], sum_send.at[number, index])
        return carry

    lax.fori_loop(0, SLABS, finish, 0)
    out_ref[...] = returned[...]


def experts(outbound, gate_weight, up_weight, down_weight):
    width, units = gate_weight.shape[1:]
    rows = SLAB * CAP
    tile_rows = outbound.shape[0]
    shares = (SLABS, rows, width)
    flat = pltpu.VMEM((tile_rows, LANES), jnp.bfloat16)
    share = pltpu.VMEM(shares, jnp.bfloat16)
    dma = pltpu.SemaphoreType.DMA
    return pl.pallas_call(
        expert_kernel,
        out_shape=jax.ShapeDtypeStruct(outbound.shape, jnp.bfloat16),
        in_specs=[pl.BlockSpec(memory_space=pltpu.VMEM)]
        + [pl.BlockSpec(memory_space=pl.ANY)] * 3,
        out_specs=pl.BlockSpec(memory_space=pltpu.VMEM),
        scratch_shapes=[
            pltpu.VMEM((width, units), jnp.bfloat16),
            pltpu.VMEM((width, units), jnp.bfloat16),
            pltpu.VMEM((units, width), jnp.bfloat16),
            flat,
            pltpu.VMEM((SLABS, 4 * rows, width), jnp.bfloat16),
            pltpu.VMEM((HELD, 4 * rows, width), jnp.float32),
            share,
            share,
            share,
            share,
            share,
            share,
            flat,
            flat,
            pltpu.VMEM((tile_rows // SLABS, LANES), jnp.float32),
            dma((3,)),
            dma((SLABS,)),
            dma((SLABS,)),
            dma((SLABS, 3)),
            dma((SLABS, 4)),
            dma((SLABS, 3)),
            dma((SLABS, 3)),
            dma((SLABS,)),
            dma((SLABS,)),
        ],
        compiler_params=pltpu.CompilerParams(
            collective_id=0, has_side_effects=True, vmem_limit_bytes=60 * 1024 * 1024
        ),
        cost_estimate=pl.CostEstimate(
            flops=8 * tile_rows * LANES * units * 3, bytes_accessed=10**7, transcendentals=10**6
        ),
        name="experts",
    )(outbound, gate_weight, up_weight, down_weight)


def attend_kernel(blocks, q_ref, kv_ref, out_ref):
    part = pl.program_id(0)
    heads, half, width = q_ref.shape[1:]
    span = 2 * half
    stride = span + 16
    rows = heads * half
    last = blocks[part]
    q = q_ref[0].reshape(rows, width)
    key_at = lax.broadcasted_iota(jnp.int32, (span, span), 0)
    out_at = lax.broadcasted_iota(jnp.int32, (span, span), 1)
    tri = (key_at >= out_at).astype(jnp.bfloat16)
    scale = LOG2E / math.sqrt(width)

    def scored(block):
        start = pl.multiple_of(block * stride, 16)
        k = kv_ref[pl.ds(start, span), :width]
        raw = lax.dot_general(q, k, (((1,), (1,)), ((), ())), preferred_element_type=jnp.float32)
        terms = kv_ref[pl.ds(start + span, 16), :].astype(jnp.float32) * LOG2E
        bias = jnp.concatenate(
            [jnp.broadcast_to(terms[h : h + 1], (half, span)) for h in range(heads)], axis=0
        )
        return raw * scale + bias

    def summed(scores, earlier):
        soft = jnp.maximum(scores, 0.0) + jnp.log2(1.0 + jnp.exp2(-jnp.abs(scores)))
        if earlier is not None:
            soft = jnp.where(earlier, soft, 0.0)
        high = soft.astype(jnp.bfloat16)
        low = (soft - high.astype(jnp.float32)).astype(jnp.bfloat16)
        return jnp.dot(high, tri, preferred_element_type=jnp.float32) + jnp.dot(
            low, tri, preferred_element_type=jnp.float32
        )

    def added(block, scores, sums, accum, carried, earlier):
        weights = jnp.exp2(scores - sums - carried)
        if earlier is not None:
            weights = jnp.where(earlier, weights, 0.0)
        v = kv_ref[pl.ds(pl.multiple_of(block * stride, 16), span), width:]
        accum = accum + jnp.dot(
            weights.astype(jnp.bfloat16), v, preferred_element_type=jnp.float32
        )
        return accum, carried + sums[:, :1]

    def one(block, state, earlier=None):
        scores = scored(block)
        return added(block, scores, summed(scores, earlier), *state, earlier)

    def two(block, state):
        first, second = scored(block), scored(block - 1)
        first_sums, second_sums = summed(first, None), summed(second, None)
        state = added(block, first, first_sums, *state, None)
        return added(block - 1, second, second_sums, *state, None)

    row_at = lax.broadcasted_iota(jnp.int32, (rows, span), 0) % half + part * half
    earlier = lax.broadcasted_iota(jnp.int32, (rows, span), 1) < row_at
    state = (jnp.zeros((rows, width), jnp.float32), jnp.zeros((rows, 1), jnp.float32))
    state = one(last, state, earlier)
    odd = last % 2
    state = lax.fori_loop(0, odd, lambda i, st: one(last - 1, st), state)
    state = lax.fori_loop(0, last // 2, lambda i, st: two(last - odd - 1 - 2 * i, st), state)
    for h in range(heads):
        out_ref[0, :, h * width : (h + 1) * width] = state[0][h * half : (h + 1) * half].astype(
            jnp.bfloat16
        )


def attend(parts, kv_all, blocks):
    count, heads, half, width = parts.shape
    grid_spec = pltpu.PrefetchScalarGridSpec(
        num_scalar_prefetch=1,
        grid=(count,),
        in_specs=[
            pl.BlockSpec((1, heads, half, width), lambda p, b: (p, 0, 0, 0)),
            pl.BlockSpec(kv_all.shape, lambda p, b: (0, 0), pipeline_mode=pl.Buffered(1)),
        ],
        out_specs=pl.BlockSpec((1, half, heads * width), lambda p, b: (p, 0, 0)),
    )
    pairs = kv_all.shape[0] * heads * half
    return pl.pallas_call(
        attend_kernel,
        grid_spec=grid_spec,
        out_shape=jax.ShapeDtypeStruct((count, half, heads * width), jnp.bfloat16),
        compiler_params=pltpu.CompilerParams(vmem_limit_bytes=40 * 1024 * 1024),
        cost_estimate=pl.CostEstimate(
            flops=pairs * 2048, bytes_accessed=kv_all.size * 2, transcendentals=pairs * 3
        ),
    )(blocks, parts, kv_all)


def body(
    queries,
    keys,
    values,
    key_bias,
    out_weight,
    tokens_b,
    moe_gain,
    gate_weight,
    up_weight,
    down_weight,
    routes,
    route_weights,
):
    tok_rows, local_heads, head_dim = queries.shape
    ep_count = lax.axis_size("ep")
    kv_all = gathered_keys(keys, values, key_bias, "ep")
    device_ep = lax.axis_index("ep")
    half_rows = tok_rows // 2
    by_head = jnp.transpose(queries, (1, 0, 2))
    handed = mirrored(by_head[:, half_rows:], "ep")
    place = jnp.stack((device_ep // SLAB, device_ep % SLAB)).astype(jnp.int32)
    outbound, places = packed(tokens_b, moe_gain, routes, place)
    returned = experts(outbound, gate_weight, up_weight, down_weight)
    halves = jnp.stack((by_head[:, :half_rows], handed))
    halves, returned = lax.optimization_barrier((halves, returned))
    blocks = jnp.stack((device_ep, ep_count - 1 - device_ep)).astype(jnp.int32)
    parts = attend(halves, kv_all, blocks)
    attended = jnp.concatenate((parts[0], mirrored(parts[1], "ep")), axis=0)
    moe_out = combined(returned, places, route_weights.reshape(-1), tokens_b.shape[1])
    mixed_sum = summed_on_arrival(
        jnp.dot(attended, out_weight, preferred_element_type=jnp.float32).astype(jnp.bfloat16),
        "tp",
        0,
    ).astype(jnp.bfloat16)
    return (mixed_sum, moe_out)


def solution(mesh):
    in_specs = (
        P("ep", "tp", None),
        P("ep", "tp", None),
        P("ep", "tp", None),
        P("ep", "tp"),
        P("tp", None),
        P(("ep", "tp"), None),
        P(),
        P("ep", None, "tp"),
        P("ep", None, "tp"),
        P("ep", "tp", None),
        P(("ep", "tp"), None),
        P(("ep", "tp"), None),
    )
    out_specs = (P(("ep", "tp"), None), P(("ep", "tp"), None))
    return jax.shard_map(body, mesh=mesh, in_specs=in_specs, out_specs=out_specs, check_vma=False)
```

```python
import math

import jax
import jax.numpy as jnp
from jax import lax
from jax.experimental import pallas as pl
from jax.experimental.pallas import tpu as pltpu
from jax.sharding import PartitionSpec as P

LOG2E = 1.4426950408889634
LANES = 128
SLABS = 8
SLAB = 8
TOP = 2
CAP = 6
HELD = 4
LINES = 4
AHEAD = 3
ATTEND_FROM = 7
STEPS_PER_TURN = 7
STEPS = (0, 2, -2, 4, 3, -3, 1, -1)


def key_blocks(keys, values, bias):
    rows, kv_heads, head_dim = keys.shape
    kv = jnp.concatenate((keys.reshape(rows, head_dim), values.reshape(rows, head_dim)), axis=1)
    terms = jnp.pad(bias.T, ((0, 16 - bias.shape[1]), (0, 0)))
    return jnp.concatenate((kv, terms), axis=0)


def round_step(number):
    step = 0
    for at, value in enumerate(STEPS):
        step = jnp.where(number == at, value, step)
    return step


def pack_kernel(routes, place, tokens_ref, gain_ref, out_ref, places_ref, rows_ref, counts):
    token_count, width = tokens_ref.shape
    tiles = width // LANES
    out_ref[...] = jnp.zeros_like(out_ref)
    tokens = tokens_ref[...].astype(jnp.float32)
    scale = lax.rsqrt(jnp.mean(tokens * tokens, axis=1, keepdims=True) + 1e-06)
    normed = tokens * scale * gain_ref[...].astype(jnp.float32)
    for tile in range(tiles):
        rows_ref[pl.ds(tile, token_count, stride=tiles), :] = normed[
            :, tile * LANES : (tile + 1) * LANES
        ]

    slab, spot = place[0], place[1]

    def opened(index, carry):
        number, side = index // SLAB, index % SLAB
        home = ((slab + round_step(number) + SLABS) % SLABS) * SLAB + (spot + side) % SLAB
        counts[home] = index * CAP
        return carry

    lax.fori_loop(0, counts.shape[0], opened, 0)

    def one(token, carry):
        row = rows_ref[pl.ds(pl.multiple_of(token * tiles, tiles), tiles), :].astype(jnp.bfloat16)
        for choice in range(TOP):
            expert = routes[token * TOP + choice]
            slot = counts[expert]
            counts[expert] = slot + 1
            places_ref[token * TOP + choice] = slot
            out_ref[pl.ds(pl.multiple_of(slot * tiles, tiles), tiles), :] = row
        return carry

    lax.fori_loop(0, token_count, one, 0, unroll=4)


def packed(tokens, gain, routes, place):
    token_count, width = tokens.shape
    tiles = width // LANES
    return pl.pallas_call(
        pack_kernel,
        grid_spec=pltpu.PrefetchScalarGridSpec(
            num_scalar_prefetch=2,
            grid=(1,),
            in_specs=[
                pl.BlockSpec(tokens.shape, lambda i, r, p: (0, 0)),
                pl.BlockSpec((1, width), lambda i, r, p: (0, 0)),
            ],
            out_specs=[
                pl.BlockSpec((SLABS * SLAB * CAP * tiles, LANES), lambda i, r, p: (0, 0)),
                pl.BlockSpec(memory_space=pltpu.SMEM),
            ],
            scratch_shapes=[
                pltpu.VMEM((token_count * tiles, LANES), jnp.float32),
                pltpu.SMEM((SLABS * SLAB,), jnp.int32),
            ],
        ),
        out_shape=[
            jax.ShapeDtypeStruct((SLABS * SLAB * CAP * tiles, LANES), jnp.bfloat16),
            jax.ShapeDtypeStruct((token_count * TOP,), jnp.int32),
        ],
        cost_estimate=pl.CostEstimate(flops=10**7, bytes_accessed=2 * 10**6, transcendentals=128),
        name="pack",
    )(routes.reshape(-1), place, tokens, gain.reshape(1, -1))


def combine_kernel(places, weights, returned_ref, out_ref, rows_ref):
    token_count, width = out_ref.shape
    tiles = width // LANES

    def picked(entry):
        start = pl.multiple_of(places[entry] * tiles, tiles)
        return returned_ref[pl.ds(start, tiles), :].astype(jnp.float32) * weights[entry]

    def one(token, carry):
        rows_ref[pl.ds(pl.multiple_of(token * tiles, tiles), tiles), :] = picked(
            token * TOP
        ) + picked(token * TOP + 1)
        return carry

    lax.fori_loop(0, token_count, one, 0, unroll=4)
    for tile in range(tiles):
        out_ref[:, tile * LANES : (tile + 1) * LANES] = rows_ref[
            pl.ds(tile, token_count, stride=tiles), :
        ].astype(jnp.bfloat16)


def combined(returned, places, weights, width):
    token_count = places.shape[0] // TOP
    tiles = width // LANES
    return pl.pallas_call(
        combine_kernel,
        grid_spec=pltpu.PrefetchScalarGridSpec(
            num_scalar_prefetch=2,
            grid=(1,),
            in_specs=[pl.BlockSpec(returned.shape, lambda i, p, w: (0, 0))],
            out_specs=pl.BlockSpec((token_count, width), lambda i, p, w: (0, 0)),
            scratch_shapes=[pltpu.VMEM((token_count * tiles, LANES), jnp.float32)],
        ),
        out_shape=jax.ShapeDtypeStruct((token_count, width), jnp.bfloat16),
        cost_estimate=pl.CostEstimate(flops=10**7, bytes_accessed=2 * 10**6, transcendentals=0),
        name="combine",
    )(places, weights, returned)


def attend_block_maker(kv_ref, span, stride, width, rows, locate):
    half = span // 2
    key_at = lax.broadcasted_iota(jnp.int32, (span, span), 0)
    out_at = lax.broadcasted_iota(jnp.int32, (span, span), 1)
    scale = LOG2E / math.sqrt(width)

    def scored(q, block):
        start = locate(block)
        k = kv_ref[pl.ds(start, span), :width]
        raw = lax.dot_general(q, k, (((1,), (1,)), ((), ())), preferred_element_type=jnp.float32)
        terms = kv_ref[pl.ds(start + span, 16), :].astype(jnp.float32) * LOG2E
        bias = jnp.concatenate(
            [jnp.broadcast_to(terms[h : h + 1], (half, span)) for h in range(rows // half)], axis=0
        )
        return raw * scale + bias

    def summed(scores, earlier):
        soft = jnp.maximum(scores, 0.0) + jnp.log2(1.0 + jnp.exp2(-jnp.abs(scores)))
        if earlier is not None:
            soft = jnp.where(earlier, soft, 0.0)
        high = soft.astype(jnp.bfloat16)
        low = (soft - high.astype(jnp.float32)).astype(jnp.bfloat16)
        tri = (key_at >= out_at).astype(jnp.bfloat16)
        return jnp.dot(high, tri, preferred_element_type=jnp.float32) + jnp.dot(
            low, tri, preferred_element_type=jnp.float32
        )

    def added(block, scores, sums, accum, carried, earlier):
        weights = jnp.exp2(scores - sums - carried)
        if earlier is not None:
            weights = jnp.where(earlier, weights, 0.0)
        v = kv_ref[pl.ds(locate(block), span), width:]
        accum = accum + jnp.dot(
            weights.astype(jnp.bfloat16), v, preferred_element_type=jnp.float32
        )
        return accum, carried + sums[:, :1]

    def one(q, block, state, earlier=None):
        scores = scored(q, block)
        return added(block, scores, summed(scores, earlier), *state, earlier)

    def two(q, block, state):
        first, second = scored(q, block), scored(q, block - 1)
        first_sums, second_sums = summed(first, None), summed(second, None)
        state = added(block, first, first_sums, *state, None)
        return added(block - 1, second, second_sums, *state, None)

    return one, two


def expert_kernel(
    outbound,
    kv_in,
    q_in,
    mix_hbm,
    gate_hbm,
    up_hbm,
    down_hbm,
    out_ref,
    mixed_ref,
    gate,
    up,
    down,
    arrived,
    taken,
    part,
    opp_out,
    near_out,
    far_out,
    opp_in,
    near_in,
    far_in,
    result,
    returned,
    relay,
    kv_all,
    q_both,
    att,
    att_back,
    accum,
    carried,
    mix_weight,
    mix_out,
    mix_in,
    weight_sem,
    go_send,
    go_recv,
    take_send,
    take_recv,
    sum_send,
    sum_recv,
    back_send,
    back_recv,
    col_send,
    col_recv,
    row_send,
    row_recv,
    hop_send,
    hop_recv,
    core_send,
    core_recv,
    swap_send,
    swap_recv,
    mix_send,
    mix_recv,
):
    me = lax.axis_index("ep")
    seat = lax.axis_index("tp")
    seats = lax.axis_size("tp")
    slab, spot = me // SLAB, me % SLAB
    width = down.shape[1]
    tiles = width // LANES
    block = CAP * tiles
    group = SLAB * block
    rows = SLAB * CAP

    def target(number, side):
        return ((slab + round_step(number) + SLABS) % SLABS) * SLAB + (spot + side) % SLAB

    def origin(number, side):
        return ((slab - round_step(number) + SLABS) % SLABS) * SLAB + (spot - side + SLAB) % SLAB

    def neighbour(step):
        return (seat + step + seats) % seats

    def piece(ref, number, side):
        return ref.at[pl.ds(pl.multiple_of((number * SLAB + side) * block, block), block)]

    def over_ep(source, landing, number, side, device, send, recv):
        return pltpu.make_async_remote_copy(
            src_ref=piece(source, number, side),
            dst_ref=piece(landing, number, side),
            send_sem=send.at[number],
            recv_sem=recv.at[number],
            device_id={"ep": device},
            device_id_type=pl.DeviceIdType.MESH,
        )

    def over_tp(source, landing, send, recv, step):
        return pltpu.make_async_remote_copy(
            src_ref=source,
            dst_ref=landing,
            send_sem=send,
            recv_sem=recv,
            device_id={"tp": neighbour(step)},
            device_id_type=pl.DeviceIdType.MESH,
        )

    def await_group(ref, sem, number):
        @pl.when(number == 0)
        def _():
            rest = ref.at[pl.ds(block, group - block)]
            pltpu.make_async_copy(rest, rest, sem.at[0]).wait()

        @pl.when(number > 0)
        def _():
            whole = ref.at[pl.ds(pl.multiple_of(number * group, group), group)]
            pltpu.make_async_copy(whole, whole, sem.at[number]).wait()

    def await_one(ref, sem):
        pltpu.make_async_copy(ref, ref, sem).wait()

    loads = [
        pltpu.make_async_copy(source.at[0], landing, weight_sem.at[i])
        for i, (source, landing) in enumerate(((gate_hbm, gate), (up_hbm, up), (down_hbm, down)))
    ]
    loads.append(pltpu.make_async_copy(mix_hbm, mix_weight, weight_sem.at[3]))
    for load in loads:
        load.start()

    barrier = pltpu.get_barrier_semaphore()

    def greet(index, carry):
        pl.semaphore_signal(
            barrier,
            inc=1,
            device_id={"ep": target(index // SLAB, index % SLAB)},
            device_id_type=pl.DeviceIdType.MESH,
        )
        return carry

    lax.fori_loop(1, SLABS * SLAB, greet, 0)
    for step in (-1, 1, 2):
        pl.semaphore_signal(
            barrier,
            inc=1,
            device_id={"tp": neighbour(step)},
            device_id_type=pl.DeviceIdType.MESH,
        )
    pl.semaphore_wait(barrier, SLABS * SLAB + 2)

    def dispatch(index, carry):
        number, side = index // SLAB, index % SLAB
        over_ep(
            outbound, arrived, number, side, target(number, side), go_send, go_recv
        ).start()
        return carry

    lax.fori_loop(1, AHEAD * SLAB, dispatch, 0)
    line, core = spot // 2, spot % 2
    stride, head_pair = kv_in.shape
    head_dim = head_pair // 2
    span = stride - 16
    half = span // 2
    mirror = SLABS * SLAB - 1 - me

    def kv_block(core_at, line_at, slab_at):
        at = (core_at * LINES + line_at) * SLABS + slab_at
        return kv_all.at[pl.ds(pl.multiple_of(at * stride, 16), stride)]

    def remote(source, landing, send, recv, device):
        return pltpu.make_async_remote_copy(
            src_ref=source,
            dst_ref=landing,
            send_sem=send,
            recv_sem=recv,
            device_id={"ep": device},
            device_id_type=pl.DeviceIdType.MESH,
        )

    remote(q_in.at[1], q_both.at[0], swap_send.at[0], swap_recv.at[0], mirror).start()
    for away in (1, 7, 2, 6, 3, 5, 4):
        remote(
            kv_in,
            kv_block(core, line, slab),
            col_send.at[away],
            col_recv.at[away],
            ((slab + away) % SLABS) * SLAB + spot,
        ).start()
    lax.fori_loop(AHEAD * SLAB, SLABS * SLAB, dispatch, 0)
    arrived[0:block] = outbound[0:block]
    kv_block(core, line, slab)[...] = kv_in[...]
    q_both[1] = q_in[0]

    def pair_of(number):
        first = jnp.where(number == 0, 0, SLABS - number)
        return (slab - first + SLABS) % SLABS, (slab - number - 1 + SLABS) % SLABS

    def on_line(step):
        return slab * SLAB + ((line + step + LINES) % LINES) * 2 + core

    other_core = slab * SLAB + line * 2 + 1 - core

    def to_core(number, at, line_at, slab_at):
        held = kv_block(core, line_at, slab_at)
        remote(
            held, held, core_send.at[number, at], core_recv.at[number, at], other_core
        ).start()

    def share_column(number):
        @pl.when(number > 0)
        def _():
            await_one(kv_in, col_recv.at[SLABS - number])

        await_one(kv_in, col_recv.at[number + 1])
        for which, slab_at in enumerate(pair_of(number)):
            held = kv_block(core, line, slab_at)
            for way, step in enumerate((1, -1)):
                remote(
                    held,
                    held,
                    row_send.at[number, which * 2 + way],
                    row_recv.at[number, which * 2 + way],
                    on_line(step),
                ).start()
            to_core(number, which, line, slab_at)

    def relay_column(number):
        for at in range(4):
            await_one(kv_in, row_recv.at[number, at])
        left, right = (line - 1 + LINES) % LINES, (line + 1) % LINES
        first, second = pair_of(number)
        for way, (line_at, slab_at, step) in enumerate(((left, first, 1), (right, second, -1))):
            held = kv_block(core, line_at, slab_at)
            remote(
                held,
                held,
                hop_send.at[number, way],
                hop_recv.at[number, way],
                on_line(step),
            ).start()
        for at, (line_at, slab_at) in enumerate(
            ((left, first), (left, second), (right, first), (right, second))
        ):
            to_core(number, 2 + at, line_at, slab_at)

    def close_column(number):
        far_line = (line + 2) % LINES
        for way, slab_at in enumerate(pair_of(number)):
            await_one(kv_in, hop_recv.at[number, way])
            to_core(number, 6 + way, far_line, slab_at)

    def locate(number):
        at = ((number % 2) * LINES + (number % SLAB) // 2) * SLABS + number // SLAB
        return pl.multiple_of(at * stride, 16)

    heads = q_in.shape[1] // half
    one, two = attend_block_maker(kv_all, span, stride, head_dim, heads * half, locate)
    other_steps = 1 + mirror // 2
    step_total = SLABS * SLAB // 2 + 1

    def attend_step(number, carry):
        own = jnp.where(number < other_steps, 0, 1)
        local = number - own * other_steps
        last = jnp.where(number < other_steps, mirror, me)
        odd = last % 2
        q = q_both[own]

        @pl.when(local == 0)
        def _():
            shape = (heads * half, span)
            row_at = lax.broadcasted_iota(jnp.int32, shape, 0) % half + (1 - own) * half
            earlier = lax.broadcasted_iota(jnp.int32, shape, 1) < row_at
            state = (jnp.zeros(accum.shape, jnp.float32), jnp.zeros(carried.shape, jnp.float32))
            accum[...], carried[...] = one(q, last, state, earlier)

            @pl.when(odd == 1)
            def _():
                accum[...], carried[...] = one(q, last - 1, (accum[...], carried[...]))

        @pl.when(local > 0)
        def _():
            block_at = last - odd + 1 - 2 * local
            accum[...], carried[...] = two(q, block_at, (accum[...], carried[...]))

        @pl.when(local == last // 2)
        def _():
            for h in range(heads):
                att[own, :, h * head_dim : (h + 1) * head_dim] = accum[
                    h * half : (h + 1) * half
                ].astype(jnp.bfloat16)

        @pl.when(number == other_steps - 1)
        def _():
            remote(att.at[0], att_back, swap_send.at[1], swap_recv.at[1], mirror).start()

        return carry

    def attend_some(index):
        @pl.when(index == ATTEND_FROM)
        def _():
            await_one(q_in.at[1], swap_recv.at[0])
            for number in range(SLABS // 2):
                for at in range(8):
                    await_one(kv_in, core_recv.at[number, at])

        first = (index - ATTEND_FROM) * STEPS_PER_TURN
        lax.fori_loop(first, jnp.minimum(first + STEPS_PER_TURN, step_total), attend_step, 0)

    share = mix_in.shape[1]

    def project(rows_in, at):
        mix_out[at : at + half] = jnp.dot(
            rows_in, mix_weight[...], preferred_element_type=jnp.float32
        ).astype(jnp.bfloat16)
        for dest in range(at // share, (at + half) // share):

            @pl.when(seat != dest)
            def _(dest=dest):
                slot = (seat - dest + seats) % seats - 1
                pltpu.make_async_remote_copy(
                    src_ref=mix_out.at[pl.ds(dest * share, share)],
                    dst_ref=mix_in.at[slot],
                    send_sem=mix_send.at[slot],
                    recv_sem=mix_recv.at[slot],
                    device_id={"tp": dest},
                    device_id_type=pl.DeviceIdType.MESH,
                ).start()

    for load in loads:
        load.wait()

    def seat_rows(ref, index, slot):
        return ref.at[index, pl.ds(pl.multiple_of(slot * rows, rows), rows)]

    def take(number):
        await_group(arrived, go_recv, number)
        relay[...] = arrived[pl.ds(pl.multiple_of(number * group, group), group), :].astype(
            jnp.float32
        )
        for tile in range(tiles):
            taken[number, 0:rows, tile * LANES : (tile + 1) * LANES] = relay[
                pl.ds(tile, rows, stride=tiles), :
            ].astype(jnp.bfloat16)
        for slot, step in ((1, 1), (2, -1)):
            over_tp(
                seat_rows(taken, number, 0),
                seat_rows(taken, number, slot),
                take_send.at[number, slot - 1],
                take_recv.at[number, slot],
                step,
            ).start()

    def forward(number):
        odd = number % 2
        slot = 1 + odd
        await_one(seat_rows(taken, number, slot), take_recv.at[number, slot])
        over_tp(
            seat_rows(taken, number, slot),
            seat_rows(taken, number, 3),
            take_send.at[number, 2],
            take_recv.at[number, 3],
            1 - 2 * odd,
        ).start()

    def compute(number):
        odd = number % 2
        far = 1 + odd
        await_one(seat_rows(taken, number, 3 - far), take_recv.at[number, 3 - far])
        await_one(seat_rows(taken, number, 3), take_recv.at[number, 3])
        x = taken[number]
        gated = jnp.dot(x, gate[...], preferred_element_type=jnp.float32)
        raised = jnp.dot(x, up[...], preferred_element_type=jnp.float32)
        hidden = (gated / (1.0 + jnp.exp(-gated)) * raised).astype(jnp.bfloat16)
        held = number % HELD
        for at in range(0, width, 512):
            part[held, :, at : at + 512] = jnp.dot(
                hidden, down[:, at : at + 512], preferred_element_type=jnp.float32
            )
        opp_out[number] = part[held, 3 * rows : 4 * rows].astype(jnp.bfloat16)
        over_tp(
            opp_out.at[number],
            opp_in.at[number],
            sum_send.at[number, 0],
            sum_recv.at[number, 0],
            2 * odd - 1,
        ).start()
        far_out[number] = seat_rows(part, held, 2 - odd)[...].astype(jnp.bfloat16)
        over_tp(
            far_out.at[number],
            far_in.at[number],
            sum_send.at[number, 1],
            sum_recv.at[number, 1],
            1 - 2 * odd,
        ).start()

    def pass_on(number):
        odd = number % 2
        await_one(opp_in.at[number], sum_recv.at[number, 0])
        near_out[number] = (
            seat_rows(part, number % HELD, 1 + odd)[...] + opp_in[number].astype(jnp.float32)
        ).astype(jnp.bfloat16)
        over_tp(
            near_out.at[number],
            near_in.at[number],
            sum_send.at[number, 2],
            sum_recv.at[number, 2],
            2 * odd - 1,
        ).start()

    def send_back(number):
        await_one(far_in.at[number], sum_recv.at[number, 1])
        await_one(near_in.at[number], sum_recv.at[number, 2])
        for tile in range(tiles):
            lanes = slice(tile * LANES, (tile + 1) * LANES)
            relay[pl.ds(tile, rows, stride=tiles), :] = (
                part[number % HELD, 0:rows, lanes]
                + far_in[number, :, lanes].astype(jnp.float32)
                + near_in[number, :, lanes].astype(jnp.float32)
            )
        result[pl.ds(pl.multiple_of(number * group, group), group), :] = relay[...].astype(
            jnp.bfloat16
        )

        def give(side, carry):
            over_ep(
                result, returned, number, side, origin(number, side), back_send, back_recv
            ).start()
            return carry

        lax.fori_loop(jnp.where(number == 0, 1, 0), SLAB, give, 0)

    stages = (take, forward, compute, pass_on, send_back)

    def turn(index, carry):
        for late, stage in enumerate(stages):
            number = index - late

            @pl.when(jnp.logical_and(number >= 0, number < SLABS))
            def _(stage=stage, number=number):
                stage(number)

        for late, stage in ((1, share_column), (2, relay_column), (3, close_column)):
            number = index - late

            @pl.when(jnp.logical_and(number >= 0, number < SLABS // 2))
            def _(stage=stage, number=number):
                stage(number)

        @pl.when(index >= ATTEND_FROM)
        def _():
            attend_some(index)

        return carry

    lax.fori_loop(0, SLABS + len(stages) - 1, turn, 0)
    returned[0:block] = result[0:block]
    project(att[1], 0)
    await_one(att_back, swap_recv.at[1])
    project(att_back[...], half)
    total = mix_out[pl.ds(pl.multiple_of(seat * share, share), share), :].astype(jnp.float32)
    for slot in range(3):
        await_one(mix_in.at[slot], mix_recv.at[slot])
        total = total + mix_in[slot].astype(jnp.float32)
    mixed_ref[...] = total.astype(jnp.bfloat16)
    await_one(q_in.at[1], swap_send.at[0])
    await_one(att_back, swap_send.at[1])
    for slot in range(3):
        await_one(mix_in.at[slot], mix_send.at[slot])
    for away in range(1, SLABS):
        await_one(kv_in, col_send.at[away])
    for number in range(SLABS // 2):
        for at in range(4):
            await_one(kv_in, row_send.at[number, at])
        for at in range(2):
            await_one(kv_in, hop_send.at[number, at])
        for at in range(8):
            await_one(kv_in, core_send.at[number, at])

    def finish(number, carry):
        await_group(returned, back_recv, number)
        await_group(outbound, go_send, number)
        await_group(result, back_send, number)
        for index in range(3):
            await_one(opp_out.at[number], take_send.at[number, index])
            await_one(opp_out.at[number], sum_send.at[number, index])
        return carry

    lax.fori_loop(0, SLABS, finish, 0)
    out_ref[...] = returned[...]


def experts(outbound, kv_in, q_in, out_weight, gate_weight, up_weight, down_weight):
    width, units = gate_weight.shape[1:]
    stride = kv_in.shape[0]
    half = (stride - 16) // 2
    head_dim = q_in.shape[2]
    rows = SLAB * CAP
    tile_rows = outbound.shape[0]
    shares = (SLABS, rows, width)
    flat = pltpu.VMEM((tile_rows, LANES), jnp.bfloat16)
    share = pltpu.VMEM(shares, jnp.bfloat16)
    dma = pltpu.SemaphoreType.DMA
    return pl.pallas_call(
        expert_kernel,
        out_shape=[
            jax.ShapeDtypeStruct(outbound.shape, jnp.bfloat16),
            jax.ShapeDtypeStruct((half // 2, width), jnp.bfloat16),
        ],
        in_specs=[pl.BlockSpec(memory_space=pltpu.VMEM)] * 3
        + [pl.BlockSpec(memory_space=pl.ANY)] * 4,
        out_specs=[pl.BlockSpec(memory_space=pltpu.VMEM)] * 2,
        scratch_shapes=[
            pltpu.VMEM((width, units), jnp.bfloat16),
            pltpu.VMEM((width, units), jnp.bfloat16),
            pltpu.VMEM((units, width), jnp.bfloat16),
            flat,
            pltpu.VMEM((SLABS, 4 * rows, width), jnp.bfloat16),
            pltpu.VMEM((HELD, 4 * rows, width), jnp.float32),
            share,
            share,
            share,
            share,
            share,
            share,
            flat,
            flat,
            pltpu.VMEM((tile_rows // SLABS, LANES), jnp.float32),
            pltpu.VMEM((SLABS * SLAB * stride, 2 * head_dim), jnp.bfloat16),
            pltpu.VMEM(q_in.shape, jnp.bfloat16),
            pltpu.VMEM((2, half, 2 * head_dim), jnp.bfloat16),
            pltpu.VMEM((half, 2 * head_dim), jnp.bfloat16),
            pltpu.VMEM((2 * half, head_dim), jnp.float32),
            pltpu.VMEM((2 * half, 1), jnp.float32),
            pltpu.VMEM(out_weight.shape, jnp.bfloat16),
            pltpu.VMEM((2 * half, width), jnp.bfloat16),
            pltpu.VMEM((3, half // 2, width), jnp.bfloat16),
            dma((4,)),
            dma((SLABS,)),
            dma((SLABS,)),
            dma((SLABS, 3)),
            dma((SLABS, 4)),
            dma((SLABS, 3)),
            dma((SLABS, 3)),
            dma((SLABS,)),
            dma((SLABS,)),
            dma((SLABS,)),
            dma((SLABS,)),
            dma((SLABS // 2, 4)),
            dma((SLABS // 2, 4)),
            dma((SLABS // 2, 2)),
            dma((SLABS // 2, 2)),
            dma((SLABS // 2, 8)),
            dma((SLABS // 2, 8)),
            dma((2,)),
            dma((2,)),
            dma((3,)),
            dma((3,)),
        ],
        compiler_params=pltpu.CompilerParams(
            collective_id=0, has_side_effects=True, vmem_limit_bytes=67043328
        ),
        cost_estimate=pl.CostEstimate(
            flops=8 * tile_rows * LANES * units * 3, bytes_accessed=10**7, transcendentals=10**6
        ),
        name="experts",
    )(outbound, kv_in, q_in, out_weight, gate_weight, up_weight, down_weight)


def body(
    queries,
    keys,
    values,
    key_bias,
    out_weight,
    tokens_b,
    moe_gain,
    gate_weight,
    up_weight,
    down_weight,
    routes,
    route_weights,
):
    tok_rows, local_heads, head_dim = queries.shape
    device_ep = lax.axis_index("ep")
    halves = jnp.transpose(queries.reshape(2, tok_rows // 2, local_heads, head_dim), (0, 2, 1, 3))
    place = jnp.stack((device_ep // SLAB, device_ep % SLAB)).astype(jnp.int32)
    outbound, places = packed(tokens_b, moe_gain, routes, place)
    returned, mixed_sum = experts(
        outbound,
        key_blocks(keys, values, key_bias),
        halves.reshape(2, -1, head_dim),
        out_weight,
        gate_weight,
        up_weight,
        down_weight,
    )
    moe_out = combined(returned, places, route_weights.reshape(-1), tokens_b.shape[1])
    return (mixed_sum, moe_out)


def solution(mesh):
    in_specs = (
        P("ep", "tp", None),
        P("ep", "tp", None),
        P("ep", "tp", None),
        P("ep", "tp"),
        P("tp", None),
        P(("ep", "tp"), None),
        P(),
        P("ep", None, "tp"),
        P("ep", None, "tp"),
        P("ep", "tp", None),
        P(("ep", "tp"), None),
        P(("ep", "tp"), None),
    )
    out_specs = (P(("ep", "tp"), None), P(("ep", "tp"), None))
    return jax.shard_map(body, mesh=mesh, in_specs=in_specs, out_specs=out_specs, check_vma=False)
```

```python
import math

import jax
import jax.numpy as jnp
from jax import lax
from jax.experimental import pallas as pl
from jax.experimental.pallas import tpu as pltpu
from jax.sharding import PartitionSpec as P

LOG2E = 1.4426950408889634
LANES = 128
SLABS = 8
SLAB = 8
TOP = 2
CAP = 6
HELD = 4
LINES = 4
AHEAD = 3
ATTEND_FROM = 5
STEPS_PER_TURN = 7
MIX_AT = 10
STEPS = (0, 2, -2, 4, 3, -3, 1, -1)


def key_blocks(keys, values, bias):
    rows, kv_heads, head_dim = keys.shape
    kv = jnp.concatenate((keys.reshape(rows, head_dim), values.reshape(rows, head_dim)), axis=1)
    terms = jnp.pad(bias.T, ((0, 16 - bias.shape[1]), (0, 0)))
    return jnp.concatenate((kv, terms), axis=0)


def round_step(number):
    step = 0
    for at, value in enumerate(STEPS):
        step = jnp.where(number == at, value, step)
    return step


def pack_kernel(routes, place, tokens_ref, gain_ref, out_ref, places_ref, rows_ref, counts):
    token_count, width = tokens_ref.shape
    tiles = width // LANES
    out_ref[...] = jnp.zeros_like(out_ref)
    tokens = tokens_ref[...].astype(jnp.float32)
    scale = lax.rsqrt(jnp.mean(tokens * tokens, axis=1, keepdims=True) + 1e-06)
    normed = tokens * scale
    gain = gain_ref[...].astype(jnp.float32)
    for tile in range(tiles):
        rows_ref[pl.ds(tile, token_count, stride=tiles), :] = normed[
            :, tile * LANES : (tile + 1) * LANES
        ]

    slab, spot = place[0], place[1]

    def opened(index, carry):
        number, side = index // SLAB, index % SLAB
        home = ((slab + round_step(number) + SLABS) % SLABS) * SLAB + (spot + side) % SLAB
        counts[home] = index * CAP
        return carry

    lax.fori_loop(0, counts.shape[0], opened, 0)

    def one(token, carry):
        row = rows_ref[pl.ds(pl.multiple_of(token * tiles, tiles), tiles), :] * gain
        row = row.astype(jnp.bfloat16)
        for choice in range(TOP):
            expert = routes[choice, token]
            slot = counts[expert]
            counts[expert] = slot + 1
            places_ref[token * TOP + choice] = slot
            out_ref[pl.ds(pl.multiple_of(slot * tiles, tiles), tiles), :] = row
        return carry

    lax.fori_loop(0, token_count, one, 0, unroll=4)


def packed(tokens, gain, routes, place):
    token_count, width = tokens.shape
    tiles = width // LANES
    return pl.pallas_call(
        pack_kernel,
        grid_spec=pltpu.PrefetchScalarGridSpec(
            num_scalar_prefetch=2,
            grid=(1,),
            in_specs=[
                pl.BlockSpec(tokens.shape, lambda i, r, p: (0, 0)),
                pl.BlockSpec((tiles, LANES), lambda i, r, p: (0, 0)),
            ],
            out_specs=[
                pl.BlockSpec((SLABS * SLAB * CAP * tiles, LANES), lambda i, r, p: (0, 0)),
                pl.BlockSpec(memory_space=pltpu.SMEM),
            ],
            scratch_shapes=[
                pltpu.VMEM((token_count * tiles, LANES), jnp.float32),
                pltpu.SMEM((SLABS * SLAB,), jnp.int32),
            ],
        ),
        out_shape=[
            jax.ShapeDtypeStruct((SLABS * SLAB * CAP * tiles, LANES), jnp.bfloat16),
            jax.ShapeDtypeStruct((token_count * TOP,), jnp.int32),
        ],
        cost_estimate=pl.CostEstimate(flops=10**7, bytes_accessed=2 * 10**6, transcendentals=128),
        name="pack",
    )(routes.T, place, tokens, gain.reshape(tiles, LANES))


def combine_kernel(places, weights, returned_ref, out_ref, rows_ref):
    token_count, width = out_ref.shape
    tiles = width // LANES

    def picked(token, choice):
        start = pl.multiple_of(places[token * TOP + choice] * tiles, tiles)
        return returned_ref[pl.ds(start, tiles), :].astype(jnp.float32) * weights[choice, token]

    def one(token, carry):
        rows_ref[pl.ds(pl.multiple_of(token * tiles, tiles), tiles), :] = picked(
            token, 0
        ) + picked(token, 1)
        return carry

    lax.fori_loop(0, token_count, one, 0, unroll=4)
    for tile in range(tiles):
        out_ref[:, tile * LANES : (tile + 1) * LANES] = rows_ref[
            pl.ds(tile, token_count, stride=tiles), :
        ].astype(jnp.bfloat16)


def combined(returned, places, weights, width):
    token_count = places.shape[0] // TOP
    tiles = width // LANES
    return pl.pallas_call(
        combine_kernel,
        grid_spec=pltpu.PrefetchScalarGridSpec(
            num_scalar_prefetch=2,
            grid=(1,),
            in_specs=[pl.BlockSpec(returned.shape, lambda i, p, w: (0, 0))],
            out_specs=pl.BlockSpec((token_count, width), lambda i, p, w: (0, 0)),
            scratch_shapes=[pltpu.VMEM((token_count * tiles, LANES), jnp.float32)],
        ),
        out_shape=jax.ShapeDtypeStruct((token_count, width), jnp.bfloat16),
        cost_estimate=pl.CostEstimate(flops=10**7, bytes_accessed=2 * 10**6, transcendentals=0),
        name="combine",
    )(places, weights, returned)


def attend_block_maker(kv_ref, span, stride, width, rows, locate):
    half = span // 2
    key_at = lax.broadcasted_iota(jnp.int32, (span, span), 0)
    out_at = lax.broadcasted_iota(jnp.int32, (span, span), 1)
    scale = LOG2E / math.sqrt(width)

    def scored(q, block):
        start = locate(block)
        k = kv_ref[pl.ds(start, span), :width]
        raw = lax.dot_general(q, k, (((1,), (1,)), ((), ())), preferred_element_type=jnp.float32)
        terms = kv_ref[pl.ds(start + span, 16), :].astype(jnp.float32) * LOG2E
        bias = jnp.concatenate(
            [jnp.broadcast_to(terms[h : h + 1], (half, span)) for h in range(rows // half)], axis=0
        )
        return raw * scale + bias

    def summed(scores, earlier):
        soft = jnp.maximum(scores, 0.0) + jnp.log2(1.0 + jnp.exp2(-jnp.abs(scores)))
        if earlier is not None:
            soft = jnp.where(earlier, soft, 0.0)
        high = soft.astype(jnp.bfloat16)
        low = (soft - high.astype(jnp.float32)).astype(jnp.bfloat16)
        tri = (key_at >= out_at).astype(jnp.bfloat16)
        return jnp.dot(high, tri, preferred_element_type=jnp.float32) + jnp.dot(
            low, tri, preferred_element_type=jnp.float32
        )

    def added(block, scores, sums, accum, carried, earlier):
        weights = jnp.exp2(scores - sums - carried)
        if earlier is not None:
            weights = jnp.where(earlier, weights, 0.0)
        v = kv_ref[pl.ds(locate(block), span), width:]
        accum = accum + jnp.dot(
            weights.astype(jnp.bfloat16), v, preferred_element_type=jnp.float32
        )
        return accum, carried + sums[:, :1]

    def one(q, block, state, earlier=None):
        scores = scored(q, block)
        return added(block, scores, summed(scores, earlier), *state, earlier)

    def two(q, block, state):
        first, second = scored(q, block), scored(q, block - 1)
        first_sums, second_sums = summed(first, None), summed(second, None)
        state = added(block, first, first_sums, *state, None)
        return added(block - 1, second, second_sums, *state, None)

    return one, two


def expert_kernel(
    outbound,
    kv_in,
    q_in,
    mix_hbm,
    gate_hbm,
    up_hbm,
    down_hbm,
    out_ref,
    mixed_ref,
    gate,
    up,
    down,
    arrived,
    taken,
    part,
    opp_out,
    near_out,
    far_out,
    opp_in,
    near_in,
    far_in,
    result,
    returned,
    relay,
    kv_all,
    q_both,
    att,
    att_back,
    accum,
    carried,
    mix_weight,
    mix_out,
    mix_in,
    mix_opp,
    mix_near,
    weight_sem,
    go_send,
    go_recv,
    take_send,
    take_recv,
    sum_send,
    sum_recv,
    back_send,
    back_recv,
    col_send,
    col_recv,
    row_send,
    row_recv,
    hop_send,
    hop_recv,
    core_send,
    core_recv,
    swap_send,
    swap_recv,
    mix_send,
    mix_recv,
):
    me = lax.axis_index("ep")
    seat = lax.axis_index("tp")
    seats = lax.axis_size("tp")
    slab, spot = me // SLAB, me % SLAB
    width = down.shape[1]
    tiles = width // LANES
    block = CAP * tiles
    group = SLAB * block
    rows = SLAB * CAP

    def target(number, side):
        return ((slab + round_step(number) + SLABS) % SLABS) * SLAB + (spot + side) % SLAB

    def origin(number, side):
        return ((slab - round_step(number) + SLABS) % SLABS) * SLAB + (spot - side + SLAB) % SLAB

    def neighbour(step):
        return (seat + step + seats) % seats

    def piece(ref, number, side):
        return ref.at[pl.ds(pl.multiple_of((number * SLAB + side) * block, block), block)]

    def over_ep(source, landing, number, side, device, send, recv):
        return pltpu.make_async_remote_copy(
            src_ref=piece(source, number, side),
            dst_ref=piece(landing, number, side),
            send_sem=send.at[number],
            recv_sem=recv.at[number],
            device_id={"ep": device},
            device_id_type=pl.DeviceIdType.MESH,
        )

    def over_tp(source, landing, send, recv, step):
        return pltpu.make_async_remote_copy(
            src_ref=source,
            dst_ref=landing,
            send_sem=send,
            recv_sem=recv,
            device_id={"tp": neighbour(step)},
            device_id_type=pl.DeviceIdType.MESH,
        )

    def await_group(ref, sem, number):
        @pl.when(number == 0)
        def _():
            rest = ref.at[pl.ds(block, group - block)]
            pltpu.make_async_copy(rest, rest, sem.at[0]).wait()

        @pl.when(number > 0)
        def _():
            whole = ref.at[pl.ds(pl.multiple_of(number * group, group), group)]
            pltpu.make_async_copy(whole, whole, sem.at[number]).wait()

    def await_one(ref, sem):
        pltpu.make_async_copy(ref, ref, sem).wait()

    loads = [
        pltpu.make_async_copy(source.at[0], landing, weight_sem.at[i])
        for i, (source, landing) in enumerate(((gate_hbm, gate), (up_hbm, up), (down_hbm, down)))
    ]
    loads.append(pltpu.make_async_copy(mix_hbm, mix_weight, weight_sem.at[3]))
    for load in loads:
        load.start()

    barrier = pltpu.get_barrier_semaphore()

    def greet(index, carry):
        pl.semaphore_signal(
            barrier,
            inc=1,
            device_id={"ep": target(index // SLAB, index % SLAB)},
            device_id_type=pl.DeviceIdType.MESH,
        )
        return carry

    lax.fori_loop(1, SLABS * SLAB, greet, 0)
    for step in (-1, 1):
        pl.semaphore_signal(
            barrier,
            inc=1,
            device_id={"tp": neighbour(step)},
            device_id_type=pl.DeviceIdType.MESH,
        )
    pl.semaphore_wait(barrier, SLABS * SLAB + 1)

    def dispatch(index, carry):
        number, side = index // SLAB, index % SLAB
        over_ep(
            outbound, arrived, number, side, target(number, side), go_send, go_recv
        ).start()
        return carry

    lax.fori_loop(1, AHEAD * SLAB, dispatch, 0)
    line, core = spot // 2, spot % 2
    stride, head_pair = kv_in.shape
    head_dim = head_pair // 2
    span = stride - 16
    half = span // 2
    mirror = SLABS * SLAB - 1 - me

    def kv_block(core_at, line_at, slab_at):
        at = (core_at * LINES + line_at) * SLABS + slab_at
        return kv_all.at[pl.ds(pl.multiple_of(at * stride, 16), stride)]

    def remote(source, landing, send, recv, device):
        return pltpu.make_async_remote_copy(
            src_ref=source,
            dst_ref=landing,
            send_sem=send,
            recv_sem=recv,
            device_id={"ep": device},
            device_id_type=pl.DeviceIdType.MESH,
        )

    remote(q_in.at[1], q_both.at[0], swap_send.at[0], swap_recv.at[0], mirror).start()
    for away in (1, 7, 2, 6, 3, 5, 4):
        remote(
            kv_in,
            kv_block(core, line, slab),
            col_send.at[away],
            col_recv.at[away],
            ((slab + away) % SLABS) * SLAB + spot,
        ).start()
    lax.fori_loop(AHEAD * SLAB, SLABS * SLAB, dispatch, 0)
    arrived[0:block] = outbound[0:block]
    kv_block(core, line, slab)[...] = kv_in[...]
    q_both[1] = q_in[0]

    def pair_of(number):
        first = jnp.where(number == 0, 0, SLABS - number)
        return (slab - first + SLABS) % SLABS, (slab - number - 1 + SLABS) % SLABS

    def on_line(step):
        return slab * SLAB + ((line + step + LINES) % LINES) * 2 + core

    other_core = slab * SLAB + line * 2 + 1 - core

    def to_core(number, at, line_at, slab_at):
        held = kv_block(core, line_at, slab_at)
        remote(
            held, held, core_send.at[number, at], core_recv.at[number, at], other_core
        ).start()

    def share_column(number):
        @pl.when(number > 0)
        def _():
            await_one(kv_in, col_recv.at[SLABS - number])

        await_one(kv_in, col_recv.at[number + 1])
        for which, slab_at in enumerate(pair_of(number)):
            held = kv_block(core, line, slab_at)
            for way, step in enumerate((1, -1)):
                remote(
                    held,
                    held,
                    row_send.at[number, which * 2 + way],
                    row_recv.at[number, which * 2 + way],
                    on_line(step),
                ).start()
            to_core(number, which, line, slab_at)

    def relay_column(number):
        for at in range(4):
            await_one(kv_in, row_recv.at[number, at])
        left, right = (line - 1 + LINES) % LINES, (line + 1) % LINES
        first, second = pair_of(number)
        for way, (line_at, slab_at, step) in enumerate(((left, first, 1), (right, second, -1))):
            held = kv_block(core, line_at, slab_at)
            remote(
                held,
                held,
                hop_send.at[number, way],
                hop_recv.at[number, way],
                on_line(step),
            ).start()
        for at, (line_at, slab_at) in enumerate(
            ((left, first), (left, second), (right, first), (right, second))
        ):
            to_core(number, 2 + at, line_at, slab_at)

    def close_column(number):
        far_line = (line + 2) % LINES
        for way, slab_at in enumerate(pair_of(number)):
            await_one(kv_in, hop_recv.at[number, way])
            to_core(number, 6 + way, far_line, slab_at)

    def locate(number):
        at = ((number % 2) * LINES + (number % SLAB) // 2) * SLABS + number // SLAB
        return pl.multiple_of(at * stride, 16)

    heads = q_in.shape[1] // half
    one, two = attend_block_maker(kv_all, span, stride, head_dim, heads * half, locate)
    other_steps = 1 + mirror // 2
    step_total = SLABS * SLAB // 2 + 1

    def attend_step(number, carry):
        own = jnp.where(number < other_steps, 0, 1)
        local = number - own * other_steps
        last = jnp.where(number < other_steps, mirror, me)
        odd = last % 2
        q = q_both[own]

        @pl.when(local == 0)
        def _():
            shape = (heads * half, span)
            row_at = lax.broadcasted_iota(jnp.int32, shape, 0) % half + (1 - own) * half
            earlier = lax.broadcasted_iota(jnp.int32, shape, 1) < row_at
            state = (jnp.zeros(accum.shape, jnp.float32), jnp.zeros(carried.shape, jnp.float32))
            accum[...], carried[...] = one(q, last, state, earlier)

            @pl.when(odd == 1)
            def _():
                accum[...], carried[...] = one(q, last - 1, (accum[...], carried[...]))

        @pl.when(local > 0)
        def _():
            block_at = last - odd + 1 - 2 * local
            accum[...], carried[...] = two(q, block_at, (accum[...], carried[...]))

        @pl.when(local == last // 2)
        def _():
            for h in range(heads):
                att[own, :, h * head_dim : (h + 1) * head_dim] = accum[
                    h * half : (h + 1) * half
                ].astype(jnp.bfloat16)

        @pl.when(number == other_steps - 1)
        def _():
            remote(att.at[0], att_back, swap_send.at[1], swap_recv.at[1], mirror).start()

        return carry

    def attend_some(index):
        @pl.when(index == ATTEND_FROM)
        def _():
            await_one(q_in.at[1], swap_recv.at[0])
            for number in range(SLABS // 2):
                for at in range(8):
                    await_one(kv_in, core_recv.at[number, at])

        first = (index - ATTEND_FROM) * STEPS_PER_TURN
        lax.fori_loop(first, jnp.minimum(first + STEPS_PER_TURN, step_total), attend_step, 0)

    share = mix_in.shape[1]

    def seat_share(step):
        return pl.ds(pl.multiple_of(neighbour(step) * share, share), share)

    def project():
        mix_out[0:half] = jnp.dot(
            att[1], mix_weight[...], preferred_element_type=jnp.float32
        ).astype(jnp.bfloat16)
        await_one(att_back, swap_recv.at[1])
        mix_out[half : 2 * half] = jnp.dot(
            att_back[...], mix_weight[...], preferred_element_type=jnp.float32
        ).astype(jnp.bfloat16)
        for way, step in enumerate((1, -1)):
            start = neighbour(2) * share + way * (share // 2)
            over_tp(
                mix_out.at[pl.ds(pl.multiple_of(start, share // 2), share // 2)],
                mix_opp.at[way],
                mix_send.at[way],
                mix_recv.at[way],
                step,
            ).start()

    def add_mixed():
        for way, step in enumerate((1, -1)):
            await_one(mix_opp.at[way], mix_recv.at[way])
            mix_near[way] = mix_out[seat_share(step), :]
            low = way * (share // 2)
            high = low + share // 2
            mix_near[way, low:high] = (
                mix_near[way, low:high].astype(jnp.float32) + mix_opp[way].astype(jnp.float32)
            ).astype(jnp.bfloat16)
            over_tp(
                mix_near.at[way], mix_in.at[way], mix_send.at[2 + way], mix_recv.at[2 + way], step
            ).start()

    for load in loads:
        load.wait()

    def seat_rows(ref, index, slot):
        return ref.at[index, pl.ds(pl.multiple_of(slot * rows, rows), rows)]

    def take(number):
        await_group(arrived, go_recv, number)
        relay[...] = arrived[pl.ds(pl.multiple_of(number * group, group), group), :].astype(
            jnp.float32
        )
        for tile in range(tiles):
            taken[number, 0:rows, tile * LANES : (tile + 1) * LANES] = relay[
                pl.ds(tile, rows, stride=tiles), :
            ].astype(jnp.bfloat16)
        for slot, step in ((1, 1), (2, -1)):
            over_tp(
                seat_rows(taken, number, 0),
                seat_rows(taken, number, slot),
                take_send.at[number, slot - 1],
                take_recv.at[number, slot],
                step,
            ).start()

    def forward(number):
        odd = number % 2
        slot = 1 + odd
        await_one(seat_rows(taken, number, slot), take_recv.at[number, slot])
        over_tp(
            seat_rows(taken, number, slot),
            seat_rows(taken, number, 3),
            take_send.at[number, 2],
            take_recv.at[number, 3],
            1 - 2 * odd,
        ).start()

    def compute(number):
        odd = number % 2
        far = 1 + odd
        await_one(seat_rows(taken, number, 3 - far), take_recv.at[number, 3 - far])
        await_one(seat_rows(taken, number, 3), take_recv.at[number, 3])
        x = taken[number]
        gated = jnp.dot(x, gate[...], preferred_element_type=jnp.float32)
        raised = jnp.dot(x, up[...], preferred_element_type=jnp.float32)
        hidden = (gated / (1.0 + jnp.exp(-gated)) * raised).astype(jnp.bfloat16)
        held = number % HELD
        for at in range(0, width, 512):
            part[held, :, at : at + 512] = jnp.dot(
                hidden, down[:, at : at + 512], preferred_element_type=jnp.float32
            )
        opp_out[number] = part[held, 3 * rows : 4 * rows].astype(jnp.bfloat16)
        over_tp(
            opp_out.at[number],
            opp_in.at[number],
            sum_send.at[number, 0],
            sum_recv.at[number, 0],
            2 * odd - 1,
        ).start()
        far_out[number] = seat_rows(part, held, 2 - odd)[...].astype(jnp.bfloat16)
        over_tp(
            far_out.at[number],
            far_in.at[number],
            sum_send.at[number, 1],
            sum_recv.at[number, 1],
            1 - 2 * odd,
        ).start()

    def pass_on(number):
        odd = number % 2
        await_one(opp_in.at[number], sum_recv.at[number, 0])
        near_out[number] = (
            seat_rows(part, number % HELD, 1 + odd)[...] + opp_in[number].astype(jnp.float32)
        ).astype(jnp.bfloat16)
        over_tp(
            near_out.at[number],
            near_in.at[number],
            sum_send.at[number, 2],
            sum_recv.at[number, 2],
            2 * odd - 1,
        ).start()

    def send_back(number):
        await_one(far_in.at[number], sum_recv.at[number, 1])
        await_one(near_in.at[number], sum_recv.at[number, 2])
        for tile in range(tiles):
            lanes = slice(tile * LANES, (tile + 1) * LANES)
            relay[pl.ds(tile, rows, stride=tiles), :] = (
                part[number % HELD, 0:rows, lanes]
                + far_in[number, :, lanes].astype(jnp.float32)
                + near_in[number, :, lanes].astype(jnp.float32)
            )
        result[pl.ds(pl.multiple_of(number * group, group), group), :] = relay[...].astype(
            jnp.bfloat16
        )

        def give(side, carry):
            over_ep(
                result, returned, number, side, origin(number, side), back_send, back_recv
            ).start()
            return carry

        lax.fori_loop(jnp.where(number == 0, 1, 0), SLAB, give, 0)

    stages = (take, forward, compute, pass_on, send_back)

    def turn(index, carry):
        for late, stage in enumerate(stages):
            number = index - late

            @pl.when(jnp.logical_and(number >= 0, number < SLABS))
            def _(stage=stage, number=number):
                stage(number)

        for at, stage, number in (
            (1, share_column, 0),
            (2, share_column, 1),
            (2, share_column, 2),
            (2, relay_column, 0),
            (3, share_column, 3),
            (3, relay_column, 1),
            (3, relay_column, 2),
            (3, close_column, 0),
            (4, relay_column, 3),
            (4, close_column, 1),
            (4, close_column, 2),
            (5, close_column, 3),
        ):

            @pl.when(index == at)
            def _(stage=stage, number=number):
                stage(number)

        @pl.when(index >= ATTEND_FROM)
        def _():
            attend_some(index)

        @pl.when(index == MIX_AT)
        def _():
            project()

        @pl.when(index == MIX_AT + 1)
        def _():
            add_mixed()

        return carry

    lax.fori_loop(0, SLABS + len(stages) - 1, turn, 0)
    returned[0:block] = result[0:block]
    total = mix_out[seat_share(0), :].astype(jnp.float32)
    for way in range(2):
        await_one(mix_in.at[way], mix_recv.at[2 + way])
        total = total + mix_in[way].astype(jnp.float32)
    mixed_ref[...] = total.astype(jnp.bfloat16)
    await_one(q_in.at[1], swap_send.at[0])
    await_one(att_back, swap_send.at[1])
    for way in range(2):
        await_one(mix_opp.at[way], mix_send.at[way])
        await_one(mix_in.at[way], mix_send.at[2 + way])
    for away in range(1, SLABS):
        await_one(kv_in, col_send.at[away])
    for number in range(SLABS // 2):
        for at in range(4):
            await_one(kv_in, row_send.at[number, at])
        for at in range(2):
            await_one(kv_in, hop_send.at[number, at])
        for at in range(8):
            await_one(kv_in, core_send.at[number, at])

    def finish(number, carry):
        await_group(returned, back_recv, number)
        await_group(outbound, go_send, number)
        await_group(result, back_send, number)
        for index in range(3):
            await_one(opp_out.at[number], take_send.at[number, index])
            await_one(opp_out.at[number], sum_send.at[number, index])
        return carry

    lax.fori_loop(0, SLABS, finish, 0)
    out_ref[...] = returned[...]


def experts(outbound, kv_in, q_in, out_weight, gate_weight, up_weight, down_weight):
    width, units = gate_weight.shape[1:]
    stride = kv_in.shape[0]
    half = (stride - 16) // 2
    head_dim = q_in.shape[2]
    rows = SLAB * CAP
    tile_rows = outbound.shape[0]
    shares = (SLABS, rows, width)
    flat = pltpu.VMEM((tile_rows, LANES), jnp.bfloat16)
    share = pltpu.VMEM(shares, jnp.bfloat16)
    dma = pltpu.SemaphoreType.DMA
    return pl.pallas_call(
        expert_kernel,
        out_shape=[
            jax.ShapeDtypeStruct(outbound.shape, jnp.bfloat16),
            jax.ShapeDtypeStruct((half // 2, width), jnp.bfloat16),
        ],
        in_specs=[pl.BlockSpec(memory_space=pltpu.VMEM)] * 3
        + [pl.BlockSpec(memory_space=pl.ANY)] * 4,
        out_specs=[pl.BlockSpec(memory_space=pltpu.VMEM)] * 2,
        scratch_shapes=[
            pltpu.VMEM((width, units), jnp.bfloat16),
            pltpu.VMEM((width, units), jnp.bfloat16),
            pltpu.VMEM((units, width), jnp.bfloat16),
            flat,
            pltpu.VMEM((SLABS, 4 * rows, width), jnp.bfloat16),
            pltpu.VMEM((HELD, 4 * rows, width), jnp.float32),
            share,
            share,
            share,
            share,
            share,
            share,
            flat,
            flat,
            pltpu.VMEM((tile_rows // SLABS, LANES), jnp.float32),
            pltpu.VMEM((SLABS * SLAB * stride, 2 * head_dim), jnp.bfloat16),
            pltpu.VMEM(q_in.shape, jnp.bfloat16),
            pltpu.VMEM((2, half, 2 * head_dim), jnp.bfloat16),
            pltpu.VMEM((half, 2 * head_dim), jnp.bfloat16),
            pltpu.VMEM((2 * half, head_dim), jnp.float32),
            pltpu.VMEM((2 * half, 1), jnp.float32),
            pltpu.VMEM(out_weight.shape, jnp.bfloat16),
            pltpu.VMEM((2 * half, width), jnp.bfloat16),
            pltpu.VMEM((2, half // 2, width), jnp.bfloat16),
            pltpu.VMEM((2, half // 4, width), jnp.bfloat16),
            pltpu.VMEM((2, half // 2, width), jnp.bfloat16),
            dma((4,)),
            dma((SLABS,)),
            dma((SLABS,)),
            dma((SLABS, 3)),
            dma((SLABS, 4)),
            dma((SLABS, 3)),
            dma((SLABS, 3)),
            dma((SLABS,)),
            dma((SLABS,)),
            dma((SLABS,)),
            dma((SLABS,)),
            dma((SLABS // 2, 4)),
            dma((SLABS // 2, 4)),
            dma((SLABS // 2, 2)),
            dma((SLABS // 2, 2)),
            dma((SLABS // 2, 8)),
            dma((SLABS // 2, 8)),
            dma((2,)),
            dma((2,)),
            dma((4,)),
            dma((4,)),
        ],
        compiler_params=pltpu.CompilerParams(
            collective_id=0, has_side_effects=True, vmem_limit_bytes=67043328
        ),
        cost_estimate=pl.CostEstimate(
            flops=8 * tile_rows * LANES * units * 3, bytes_accessed=10**7, transcendentals=10**6
        ),
        name="experts",
    )(outbound, kv_in, q_in, out_weight, gate_weight, up_weight, down_weight)


def body(
    queries,
    keys,
    values,
    key_bias,
    out_weight,
    tokens_b,
    moe_gain,
    gate_weight,
    up_weight,
    down_weight,
    routes,
    route_weights,
):
    tok_rows, local_heads, head_dim = queries.shape
    device_ep = lax.axis_index("ep")
    halves = jnp.transpose(queries.reshape(2, tok_rows // 2, local_heads, head_dim), (0, 2, 1, 3))
    place = jnp.stack((device_ep // SLAB, device_ep % SLAB)).astype(jnp.int32)
    outbound, places = packed(tokens_b, moe_gain, routes, place)
    returned, mixed_sum = experts(
        outbound,
        key_blocks(keys, values, key_bias),
        halves.reshape(2, -1, head_dim),
        out_weight,
        gate_weight,
        up_weight,
        down_weight,
    )
    moe_out = combined(returned, places, route_weights.T, tokens_b.shape[1])
    return (mixed_sum, moe_out)


def solution(mesh):
    in_specs = (
        P("ep", "tp", None),
        P("ep", "tp", None),
        P("ep", "tp", None),
        P("ep", "tp"),
        P("tp", None),
        P(("ep", "tp"), None),
        P(),
        P("ep", None, "tp"),
        P("ep", None, "tp"),
        P("ep", "tp", None),
        P(("ep", "tp"), None),
        P(("ep", "tp"), None),
    )
    out_specs = (P(("ep", "tp"), None), P(("ep", "tp"), None))
    return jax.shard_map(body, mesh=mesh, in_specs=in_specs, out_specs=out_specs, check_vma=False)
```

```python
import math

import jax
import jax.numpy as jnp
from jax import lax
from jax.experimental import pallas as pl
from jax.experimental.pallas import tpu as pltpu
from jax.sharding import PartitionSpec as P

LOG2E = 1.4426950408889634
LANES = 128
SLABS = 8
SLAB = 8
TOP = 2
CAP = 6
HELD = 4
LINES = 4
AHEAD = 3
ATTEND_FROM = 5
STEPS_PER_TURN = 7
MIX_AT = 10
STEPS = (0, 2, -2, 4, 3, -3, 1, -1)


def key_blocks(keys, values, bias):
    rows, kv_heads, head_dim = keys.shape
    kv = jnp.concatenate((keys.reshape(rows, head_dim), values.reshape(rows, head_dim)), axis=1)
    terms = jnp.pad(bias.T, ((0, 16 - bias.shape[1]), (0, 0)))
    return jnp.concatenate((kv, terms), axis=0)


def round_step(number):
    step = 0
    for at, value in enumerate(STEPS):
        step = jnp.where(number == at, value, step)
    return step


def pack_kernel(routes, place, tokens_ref, gain_ref, out_ref, places_ref, rows_ref, counts):
    token_count, width = tokens_ref.shape
    tiles = width // LANES
    out_ref[...] = jnp.zeros_like(out_ref)
    tokens = tokens_ref[...].astype(jnp.float32)
    scale = lax.rsqrt(jnp.mean(tokens * tokens, axis=1, keepdims=True) + 1e-06)
    normed = tokens * scale
    gain = gain_ref[...].astype(jnp.float32)
    for tile in range(tiles):
        rows_ref[pl.ds(tile, token_count, stride=tiles), :] = normed[
            :, tile * LANES : (tile + 1) * LANES
        ]

    slab, spot = place[0], place[1]

    def opened(index, carry):
        number, side = index // SLAB, index % SLAB
        home = ((slab + round_step(number) + SLABS) % SLABS) * SLAB + (spot + side) % SLAB
        counts[home] = index * CAP
        return carry

    lax.fori_loop(0, counts.shape[0], opened, 0)

    def one(token, carry):
        row = rows_ref[pl.ds(pl.multiple_of(token * tiles, tiles), tiles), :] * gain
        row = row.astype(jnp.bfloat16)
        for choice in range(TOP):
            expert = routes[choice, token]
            slot = counts[expert]
            counts[expert] = slot + 1
            places_ref[token * TOP + choice] = slot
            out_ref[pl.ds(pl.multiple_of(slot * tiles, tiles), tiles), :] = row
        return carry

    lax.fori_loop(0, token_count, one, 0, unroll=4)


def packed(tokens, gain, routes, place):
    token_count, width = tokens.shape
    tiles = width // LANES
    return pl.pallas_call(
        pack_kernel,
        grid_spec=pltpu.PrefetchScalarGridSpec(
            num_scalar_prefetch=2,
            grid=(1,),
            in_specs=[
                pl.BlockSpec(tokens.shape, lambda i, r, p: (0, 0)),
                pl.BlockSpec((tiles, LANES), lambda i, r, p: (0, 0)),
            ],
            out_specs=[
                pl.BlockSpec((SLABS * SLAB * CAP * tiles, LANES), lambda i, r, p: (0, 0)),
                pl.BlockSpec(memory_space=pltpu.SMEM),
            ],
            scratch_shapes=[
                pltpu.VMEM((token_count * tiles, LANES), jnp.float32),
                pltpu.SMEM((SLABS * SLAB,), jnp.int32),
            ],
        ),
        out_shape=[
            jax.ShapeDtypeStruct((SLABS * SLAB * CAP * tiles, LANES), jnp.bfloat16),
            jax.ShapeDtypeStruct((token_count * TOP,), jnp.int32),
        ],
        cost_estimate=pl.CostEstimate(flops=10**7, bytes_accessed=2 * 10**6, transcendentals=128),
        name="pack",
    )(routes.T, place, tokens, gain.reshape(tiles, LANES))


def combine_kernel(places, weights, returned_ref, out_ref, rows_ref):
    token_count, width = out_ref.shape
    tiles = width // LANES

    def picked(token, choice):
        start = pl.multiple_of(places[token * TOP + choice] * tiles, tiles)
        return returned_ref[pl.ds(start, tiles), :].astype(jnp.float32) * weights[choice, token]

    def one(token, carry):
        rows_ref[pl.ds(pl.multiple_of(token * tiles, tiles), tiles), :] = picked(
            token, 0
        ) + picked(token, 1)
        return carry

    lax.fori_loop(0, token_count, one, 0, unroll=4)
    for tile in range(tiles):
        out_ref[:, tile * LANES : (tile + 1) * LANES] = rows_ref[
            pl.ds(tile, token_count, stride=tiles), :
        ].astype(jnp.bfloat16)


def combined(returned, places, weights, width):
    token_count = places.shape[0] // TOP
    tiles = width // LANES
    return pl.pallas_call(
        combine_kernel,
        grid_spec=pltpu.PrefetchScalarGridSpec(
            num_scalar_prefetch=2,
            grid=(1,),
            in_specs=[pl.BlockSpec(returned.shape, lambda i, p, w: (0, 0))],
            out_specs=pl.BlockSpec((token_count, width), lambda i, p, w: (0, 0)),
            scratch_shapes=[pltpu.VMEM((token_count * tiles, LANES), jnp.float32)],
        ),
        out_shape=jax.ShapeDtypeStruct((token_count, width), jnp.bfloat16),
        cost_estimate=pl.CostEstimate(flops=10**7, bytes_accessed=2 * 10**6, transcendentals=0),
        name="combine",
    )(places, weights, returned)


def attend_block_maker(kv_ref, span, stride, width, rows, locate):
    half = span // 2
    key_at = lax.broadcasted_iota(jnp.int32, (span, span), 0)
    out_at = lax.broadcasted_iota(jnp.int32, (span, span), 1)
    scale = LOG2E / math.sqrt(width)

    def scored(q, block):
        start = locate(block)
        k = kv_ref[pl.ds(start, span), :width]
        raw = lax.dot_general(q, k, (((1,), (1,)), ((), ())), preferred_element_type=jnp.float32)
        terms = kv_ref[pl.ds(start + span, 16), :].astype(jnp.float32) * LOG2E
        bias = jnp.concatenate(
            [jnp.broadcast_to(terms[h : h + 1], (half, span)) for h in range(rows // half)], axis=0
        )
        return raw * scale + bias

    def summed(scores, earlier):
        soft = jnp.maximum(scores, 0.0) + jnp.log2(1.0 + jnp.exp2(-jnp.abs(scores)))
        if earlier is not None:
            soft = jnp.where(earlier, soft, 0.0)
        high = soft.astype(jnp.bfloat16)
        low = (soft - high.astype(jnp.float32)).astype(jnp.bfloat16)
        tri = (key_at >= out_at).astype(jnp.bfloat16)
        return jnp.dot(high, tri, preferred_element_type=jnp.float32) + jnp.dot(
            low, tri, preferred_element_type=jnp.float32
        )

    def added(block, scores, sums, accum, carried, earlier):
        weights = jnp.exp2(scores - sums - carried)
        if earlier is not None:
            weights = jnp.where(earlier, weights, 0.0)
        v = kv_ref[pl.ds(locate(block), span), width:]
        accum = accum + jnp.dot(
            weights.astype(jnp.bfloat16), v, preferred_element_type=jnp.float32
        )
        return accum, carried + sums[:, :1]

    def one(q, block, state, earlier=None):
        scores = scored(q, block)
        return added(block, scores, summed(scores, earlier), *state, earlier)

    def two(q, block, state):
        first, second = scored(q, block), scored(q, block - 1)
        first_sums, second_sums = summed(first, None), summed(second, None)
        state = added(block, first, first_sums, *state, None)
        return added(block - 1, second, second_sums, *state, None)

    return one, two


def expert_kernel(
    outbound,
    kv_in,
    q_in,
    mix_hbm,
    gate_hbm,
    up_hbm,
    down_hbm,
    out_ref,
    mixed_ref,
    gate,
    up,
    down,
    arrived,
    taken,
    part,
    opp_out,
    near_out,
    far_out,
    opp_in,
    near_in,
    far_in,
    result,
    returned,
    relay,
    kv_all,
    q_both,
    att,
    att_back,
    accum,
    carried,
    mix_weight,
    mix_out,
    mix_in,
    mix_opp,
    mix_near,
    weight_sem,
    go_send,
    go_recv,
    take_send,
    take_recv,
    sum_send,
    sum_recv,
    back_send,
    back_recv,
    col_send,
    col_recv,
    row_send,
    row_recv,
    hop_send,
    hop_recv,
    core_send,
    core_recv,
    swap_send,
    swap_recv,
    mix_send,
    mix_recv,
):
    me = lax.axis_index("ep")
    seat = lax.axis_index("tp")
    seats = lax.axis_size("tp")
    slab, spot = me // SLAB, me % SLAB
    width = down.shape[1]
    tiles = width // LANES
    block = CAP * tiles
    group = SLAB * block
    rows = SLAB * CAP

    def target(number, side):
        return ((slab + round_step(number) + SLABS) % SLABS) * SLAB + (spot + side) % SLAB

    def origin(number, side):
        return ((slab - round_step(number) + SLABS) % SLABS) * SLAB + (spot - side + SLAB) % SLAB

    def neighbour(step):
        return (seat + step + seats) % seats

    def piece(ref, number, side):
        return ref.at[pl.ds(pl.multiple_of((number * SLAB + side) * block, block), block)]

    def over_ep(source, landing, number, side, device, send, recv):
        return pltpu.make_async_remote_copy(
            src_ref=piece(source, number, side),
            dst_ref=piece(landing, number, side),
            send_sem=send.at[number],
            recv_sem=recv.at[number],
            device_id={"ep": device},
            device_id_type=pl.DeviceIdType.MESH,
        )

    def over_tp(source, landing, send, recv, step):
        return pltpu.make_async_remote_copy(
            src_ref=source,
            dst_ref=landing,
            send_sem=send,
            recv_sem=recv,
            device_id={"tp": neighbour(step)},
            device_id_type=pl.DeviceIdType.MESH,
        )

    def await_group(ref, sem, number):
        @pl.when(number == 0)
        def _():
            rest = ref.at[pl.ds(block, group - block)]
            pltpu.make_async_copy(rest, rest, sem.at[0]).wait()

        @pl.when(number > 0)
        def _():
            whole = ref.at[pl.ds(pl.multiple_of(number * group, group), group)]
            pltpu.make_async_copy(whole, whole, sem.at[number]).wait()

    def await_one(ref, sem):
        pltpu.make_async_copy(ref, ref, sem).wait()

    loads = [
        pltpu.make_async_copy(source.at[0], landing, weight_sem.at[i])
        for i, (source, landing) in enumerate(((gate_hbm, gate), (up_hbm, up), (down_hbm, down)))
    ]
    loads.append(pltpu.make_async_copy(mix_hbm, mix_weight, weight_sem.at[3]))
    for load in loads:
        load.start()

    barrier = pltpu.get_barrier_semaphore()

    def greet(index, carry):
        pl.semaphore_signal(
            barrier,
            inc=1,
            device_id={"ep": target(index // SLAB, index % SLAB)},
            device_id_type=pl.DeviceIdType.MESH,
        )
        return carry

    lax.fori_loop(1, SLABS * SLAB, greet, 0)
    for step in (-1, 1):
        pl.semaphore_signal(
            barrier,
            inc=1,
            device_id={"tp": neighbour(step)},
            device_id_type=pl.DeviceIdType.MESH,
        )
    pl.semaphore_wait(barrier, SLABS * SLAB + 1)

    def dispatch(index, carry):
        number, side = index // SLAB, index % SLAB
        over_ep(
            outbound, arrived, number, side, target(number, side), go_send, go_recv
        ).start()
        return carry

    lax.fori_loop(1, AHEAD * SLAB, dispatch, 0)
    line, core = spot // 2, spot % 2
    stride, head_pair = kv_in.shape
    head_dim = head_pair // 2
    span = stride - 16
    half = span // 2
    mirror = SLABS * SLAB - 1 - me

    def kv_block(core_at, line_at, slab_at):
        at = (core_at * LINES + line_at) * SLABS + slab_at
        return kv_all.at[pl.ds(pl.multiple_of(at * stride, 16), stride)]

    def remote(source, landing, send, recv, device):
        return pltpu.make_async_remote_copy(
            src_ref=source,
            dst_ref=landing,
            send_sem=send,
            recv_sem=recv,
            device_id={"ep": device},
            device_id_type=pl.DeviceIdType.MESH,
        )

    remote(q_in.at[1], q_both.at[0], swap_send.at[0], swap_recv.at[0], mirror).start()
    for ahead, aways in ((AHEAD + 1, (1, 7, 2, 6, 3)), (SLABS, (5, 4))):
        for away in aways:
            remote(
                kv_in,
                kv_block(core, line, slab),
                col_send.at[away],
                col_recv.at[away],
                ((slab + away) % SLABS) * SLAB + spot,
            ).start()
        begin = AHEAD if ahead < SLABS else AHEAD + 1
        lax.fori_loop(begin * SLAB, ahead * SLAB, dispatch, 0)
    arrived[0:block] = outbound[0:block]
    kv_block(core, line, slab)[...] = kv_in[...]
    q_both[1] = q_in[0]

    def pair_of(number):
        first = jnp.where(number == 0, 0, SLABS - number)
        return (slab - first + SLABS) % SLABS, (slab - number - 1 + SLABS) % SLABS

    def on_line(step):
        return slab * SLAB + ((line + step + LINES) % LINES) * 2 + core

    other_core = slab * SLAB + line * 2 + 1 - core

    def to_core(number, at, line_at, slab_at):
        held = kv_block(core, line_at, slab_at)
        remote(
            held, held, core_send.at[number, at], core_recv.at[number, at], other_core
        ).start()

    def share_column(number):
        @pl.when(number > 0)
        def _():
            await_one(kv_in, col_recv.at[SLABS - number])

        await_one(kv_in, col_recv.at[number + 1])
        for which, slab_at in enumerate(pair_of(number)):
            held = kv_block(core, line, slab_at)
            for way, step in enumerate((1, -1)):
                remote(
                    held,
                    held,
                    row_send.at[number, which * 2 + way],
                    row_recv.at[number, which * 2 + way],
                    on_line(step),
                ).start()
            to_core(number, which, line, slab_at)

    def relay_column(number):
        for at in range(4):
            await_one(kv_in, row_recv.at[number, at])
        left, right = (line - 1 + LINES) % LINES, (line + 1) % LINES
        first, second = pair_of(number)
        for way, (line_at, slab_at, step) in enumerate(((left, first, 1), (right, second, -1))):
            held = kv_block(core, line_at, slab_at)
            remote(
                held,
                held,
                hop_send.at[number, way],
                hop_recv.at[number, way],
                on_line(step),
            ).start()
        for at, (line_at, slab_at) in enumerate(
            ((left, first), (left, second), (right, first), (right, second))
        ):
            to_core(number, 2 + at, line_at, slab_at)

    def close_column(number):
        far_line = (line + 2) % LINES
        for way, slab_at in enumerate(pair_of(number)):
            await_one(kv_in, hop_recv.at[number, way])
            to_core(number, 6 + way, far_line, slab_at)

    def locate(number):
        at = ((number % 2) * LINES + (number % SLAB) // 2) * SLABS + number // SLAB
        return pl.multiple_of(at * stride, 16)

    heads = q_in.shape[1] // half
    one, two = attend_block_maker(kv_all, span, stride, head_dim, heads * half, locate)
    other_steps = 1 + mirror // 2
    step_total = SLABS * SLAB // 2 + 1

    def attend_step(number, carry):
        own = jnp.where(number < other_steps, 0, 1)
        local = number - own * other_steps
        last = jnp.where(number < other_steps, mirror, me)
        odd = last % 2
        q = q_both[own]

        @pl.when(local == 0)
        def _():
            shape = (heads * half, span)
            row_at = lax.broadcasted_iota(jnp.int32, shape, 0) % half + (1 - own) * half
            earlier = lax.broadcasted_iota(jnp.int32, shape, 1) < row_at
            state = (jnp.zeros(accum.shape, jnp.float32), jnp.zeros(carried.shape, jnp.float32))
            accum[...], carried[...] = one(q, last, state, earlier)

            @pl.when(odd == 1)
            def _():
                accum[...], carried[...] = one(q, last - 1, (accum[...], carried[...]))

        @pl.when(local > 0)
        def _():
            block_at = last - odd + 1 - 2 * local
            accum[...], carried[...] = two(q, block_at, (accum[...], carried[...]))

        @pl.when(local == last // 2)
        def _():
            for h in range(heads):
                att[own, :, h * head_dim : (h + 1) * head_dim] = accum[
                    h * half : (h + 1) * half
                ].astype(jnp.bfloat16)

        @pl.when(number == other_steps - 1)
        def _():
            remote(att.at[0], att_back, swap_send.at[1], swap_recv.at[1], mirror).start()

        return carry

    def attend_some(index):
        @pl.when(index == ATTEND_FROM)
        def _():
            await_one(q_in.at[1], swap_recv.at[0])
            for number in range(SLABS // 2):
                for at in range(8):
                    await_one(kv_in, core_recv.at[number, at])

        first = (index - ATTEND_FROM) * STEPS_PER_TURN
        lax.fori_loop(first, jnp.minimum(first + STEPS_PER_TURN, step_total), attend_step, 0)

    share = mix_in.shape[1]

    def seat_share(step):
        return pl.ds(pl.multiple_of(neighbour(step) * share, share), share)

    def project():
        mix_out[0:half] = jnp.dot(
            att[1], mix_weight[...], preferred_element_type=jnp.float32
        ).astype(jnp.bfloat16)
        await_one(att_back, swap_recv.at[1])
        mix_out[half : 2 * half] = jnp.dot(
            att_back[...], mix_weight[...], preferred_element_type=jnp.float32
        ).astype(jnp.bfloat16)
        for way, step in enumerate((1, -1)):
            start = neighbour(2) * share + way * (share // 2)
            over_tp(
                mix_out.at[pl.ds(pl.multiple_of(start, share // 2), share // 2)],
                mix_opp.at[way],
                mix_send.at[way],
                mix_recv.at[way],
                step,
            ).start()

    def add_mixed():
        for way, step in enumerate((1, -1)):
            await_one(mix_opp.at[way], mix_recv.at[way])
            mix_near[way] = mix_out[seat_share(step), :]
            low = way * (share // 2)
            high = low + share // 2
            mix_near[way, low:high] = (
                mix_near[way, low:high].astype(jnp.float32) + mix_opp[way].astype(jnp.float32)
            ).astype(jnp.bfloat16)
            over_tp(
                mix_near.at[way], mix_in.at[way], mix_send.at[2 + way], mix_recv.at[2 + way], step
            ).start()

    for load in loads:
        load.wait()

    def seat_rows(ref, index, slot):
        return ref.at[index, pl.ds(pl.multiple_of(slot * rows, rows), rows)]

    def take(number):
        await_group(arrived, go_recv, number)
        relay[...] = arrived[pl.ds(pl.multiple_of(number * group, group), group), :].astype(
            jnp.float32
        )
        for tile in range(tiles):
            taken[number, 0:rows, tile * LANES : (tile + 1) * LANES] = relay[
                pl.ds(tile, rows, stride=tiles), :
            ].astype(jnp.bfloat16)
        for slot, step in ((1, 1), (2, -1)):
            over_tp(
                seat_rows(taken, number, 0),
                seat_rows(taken, number, slot),
                take_send.at[number, slot - 1],
                take_recv.at[number, slot],
                step,
            ).start()

    def forward(number):
        odd = number % 2
        slot = 1 + odd
        await_one(seat_rows(taken, number, slot), take_recv.at[number, slot])
        over_tp(
            seat_rows(taken, number, slot),
            seat_rows(taken, number, 3),
            take_send.at[number, 2],
            take_recv.at[number, 3],
            1 - 2 * odd,
        ).start()

    def compute(number):
        odd = number % 2
        far = 1 + odd
        await_one(seat_rows(taken, number, 3 - far), take_recv.at[number, 3 - far])
        await_one(seat_rows(taken, number, 3), take_recv.at[number, 3])
        x = taken[number]
        gated = jnp.dot(x, gate[...], preferred_element_type=jnp.float32)
        raised = jnp.dot(x, up[...], preferred_element_type=jnp.float32)
        hidden = (gated / (1.0 + jnp.exp(-gated)) * raised).astype(jnp.bfloat16)
        held = number % HELD
        for at in range(0, width, 512):
            part[held, :, at : at + 512] = jnp.dot(
                hidden, down[:, at : at + 512], preferred_element_type=jnp.float32
            )
        opp_out[number] = part[held, 3 * rows : 4 * rows].astype(jnp.bfloat16)
        over_tp(
            opp_out.at[number],
            opp_in.at[number],
            sum_send.at[number, 0],
            sum_recv.at[number, 0],
            2 * odd - 1,
        ).start()
        far_out[number] = seat_rows(part, held, 2 - odd)[...].astype(jnp.bfloat16)
        over_tp(
            far_out.at[number],
            far_in.at[number],
            sum_send.at[number, 1],
            sum_recv.at[number, 1],
            1 - 2 * odd,
        ).start()

    def pass_on(number):
        odd = number % 2
        await_one(opp_in.at[number], sum_recv.at[number, 0])
        near_out[number] = (
            seat_rows(part, number % HELD, 1 + odd)[...] + opp_in[number].astype(jnp.float32)
        ).astype(jnp.bfloat16)
        over_tp(
            near_out.at[number],
            near_in.at[number],
            sum_send.at[number, 2],
            sum_recv.at[number, 2],
            2 * odd - 1,
        ).start()

    def send_back(number):
        await_one(far_in.at[number], sum_recv.at[number, 1])
        await_one(near_in.at[number], sum_recv.at[number, 2])
        for tile in range(tiles):
            lanes = slice(tile * LANES, (tile + 1) * LANES)
            relay[pl.ds(tile, rows, stride=tiles), :] = (
                part[number % HELD, 0:rows, lanes]
                + far_in[number, :, lanes].astype(jnp.float32)
                + near_in[number, :, lanes].astype(jnp.float32)
            )
        result[pl.ds(pl.multiple_of(number * group, group), group), :] = relay[...].astype(
            jnp.bfloat16
        )

        def give(side, carry):
            over_ep(
                result, returned, number, side, origin(number, side), back_send, back_recv
            ).start()
            return carry

        lax.fori_loop(jnp.where(number == 0, 1, 0), SLAB, give, 0)

    stages = (take, forward, compute, pass_on, send_back)

    def turn(index, carry):
        for late, stage in enumerate(stages):
            number = index - late

            @pl.when(jnp.logical_and(number >= 0, number < SLABS))
            def _(stage=stage, number=number):
                stage(number)

        for at, stage, number in (
            (1, share_column, 0),
            (2, share_column, 1),
            (2, share_column, 2),
            (2, relay_column, 0),
            (3, share_column, 3),
            (3, relay_column, 1),
            (3, relay_column, 2),
            (3, close_column, 0),
            (4, relay_column, 3),
            (4, close_column, 1),
            (4, close_column, 2),
            (5, close_column, 3),
        ):

            @pl.when(index == at)
            def _(stage=stage, number=number):
                stage(number)

        @pl.when(index >= ATTEND_FROM)
        def _():
            attend_some(index)

        @pl.when(index == MIX_AT)
        def _():
            project()

        @pl.when(index == MIX_AT + 1)
        def _():
            add_mixed()

        return carry

    lax.fori_loop(0, SLABS + len(stages) - 1, turn, 0)
    returned[0:block] = result[0:block]
    total = mix_out[seat_share(0), :].astype(jnp.float32)
    for way in range(2):
        await_one(mix_in.at[way], mix_recv.at[2 + way])
        total = total + mix_in[way].astype(jnp.float32)
    mixed_ref[...] = total.astype(jnp.bfloat16)
    await_one(q_in.at[1], swap_send.at[0])
    await_one(att_back, swap_send.at[1])
    for way in range(2):
        await_one(mix_opp.at[way], mix_send.at[way])
        await_one(mix_in.at[way], mix_send.at[2 + way])
    for away in range(1, SLABS):
        await_one(kv_in, col_send.at[away])
    for number in range(SLABS // 2):
        for at in range(4):
            await_one(kv_in, row_send.at[number, at])
        for at in range(2):
            await_one(kv_in, hop_send.at[number, at])
        for at in range(8):
            await_one(kv_in, core_send.at[number, at])

    def finish(number, carry):
        await_group(returned, back_recv, number)
        await_group(outbound, go_send, number)
        await_group(result, back_send, number)
        for index in range(3):
            await_one(opp_out.at[number], take_send.at[number, index])
            await_one(opp_out.at[number], sum_send.at[number, index])
        return carry

    lax.fori_loop(0, SLABS, finish, 0)
    out_ref[...] = returned[...]


def experts(outbound, kv_in, q_in, out_weight, gate_weight, up_weight, down_weight):
    width, units = gate_weight.shape[1:]
    stride = kv_in.shape[0]
    half = (stride - 16) // 2
    head_dim = q_in.shape[2]
    rows = SLAB * CAP
    tile_rows = outbound.shape[0]
    shares = (SLABS, rows, width)
    flat = pltpu.VMEM((tile_rows, LANES), jnp.bfloat16)
    share = pltpu.VMEM(shares, jnp.bfloat16)
    dma = pltpu.SemaphoreType.DMA
    return pl.pallas_call(
        expert_kernel,
        out_shape=[
            jax.ShapeDtypeStruct(outbound.shape, jnp.bfloat16),
            jax.ShapeDtypeStruct((half // 2, width), jnp.bfloat16),
        ],
        in_specs=[pl.BlockSpec(memory_space=pltpu.VMEM)] * 3
        + [pl.BlockSpec(memory_space=pl.ANY)] * 4,
        out_specs=[pl.BlockSpec(memory_space=pltpu.VMEM)] * 2,
        scratch_shapes=[
            pltpu.VMEM((width, units), jnp.bfloat16),
            pltpu.VMEM((width, units), jnp.bfloat16),
            pltpu.VMEM((units, width), jnp.bfloat16),
            flat,
            pltpu.VMEM((SLABS, 4 * rows, width), jnp.bfloat16),
            pltpu.VMEM((HELD, 4 * rows, width), jnp.float32),
            share,
            share,
            share,
            share,
            share,
            share,
            flat,
            flat,
            pltpu.VMEM((tile_rows // SLABS, LANES), jnp.float32),
            pltpu.VMEM((SLABS * SLAB * stride, 2 * head_dim), jnp.bfloat16),
            pltpu.VMEM(q_in.shape, jnp.bfloat16),
            pltpu.VMEM((2, half, 2 * head_dim), jnp.bfloat16),
            pltpu.VMEM((half, 2 * head_dim), jnp.bfloat16),
            pltpu.VMEM((2 * half, head_dim), jnp.float32),
            pltpu.VMEM((2 * half, 1), jnp.float32),
            pltpu.VMEM(out_weight.shape, jnp.bfloat16),
            pltpu.VMEM((2 * half, width), jnp.bfloat16),
            pltpu.VMEM((2, half // 2, width), jnp.bfloat16),
            pltpu.VMEM((2, half // 4, width), jnp.bfloat16),
            pltpu.VMEM((2, half // 2, width), jnp.bfloat16),
            dma((4,)),
            dma((SLABS,)),
            dma((SLABS,)),
            dma((SLABS, 3)),
            dma((SLABS, 4)),
            dma((SLABS, 3)),
            dma((SLABS, 3)),
            dma((SLABS,)),
            dma((SLABS,)),
            dma((SLABS,)),
            dma((SLABS,)),
            dma((SLABS // 2, 4)),
            dma((SLABS // 2, 4)),
            dma((SLABS // 2, 2)),
            dma((SLABS // 2, 2)),
            dma((SLABS // 2, 8)),
            dma((SLABS // 2, 8)),
            dma((2,)),
            dma((2,)),
            dma((4,)),
            dma((4,)),
        ],
        compiler_params=pltpu.CompilerParams(
            collective_id=0, has_side_effects=True, vmem_limit_bytes=67043328
        ),
        cost_estimate=pl.CostEstimate(
            flops=8 * tile_rows * LANES * units * 3, bytes_accessed=10**7, transcendentals=10**6
        ),
        name="experts",
    )(outbound, kv_in, q_in, out_weight, gate_weight, up_weight, down_weight)


def body(
    queries,
    keys,
    values,
    key_bias,
    out_weight,
    tokens_b,
    moe_gain,
    gate_weight,
    up_weight,
    down_weight,
    routes,
    route_weights,
):
    tok_rows, local_heads, head_dim = queries.shape
    device_ep = lax.axis_index("ep")
    halves = jnp.transpose(queries.reshape(2, tok_rows // 2, local_heads, head_dim), (0, 2, 1, 3))
    place = jnp.stack((device_ep // SLAB, device_ep % SLAB)).astype(jnp.int32)
    outbound, places = packed(tokens_b, moe_gain, routes, place)
    returned, mixed_sum = experts(
        outbound,
        key_blocks(keys, values, key_bias),
        halves.reshape(2, -1, head_dim),
        out_weight,
        gate_weight,
        up_weight,
        down_weight,
    )
    moe_out = combined(returned, places, route_weights.T, tokens_b.shape[1])
    return (mixed_sum, moe_out)


def solution(mesh):
    in_specs = (
        P("ep", "tp", None),
        P("ep", "tp", None),
        P("ep", "tp", None),
        P("ep", "tp"),
        P("tp", None),
        P(("ep", "tp"), None),
        P(),
        P("ep", None, "tp"),
        P("ep", None, "tp"),
        P("ep", "tp", None),
        P(("ep", "tp"), None),
        P(("ep", "tp"), None),
    )
    out_specs = (P(("ep", "tp"), None), P(("ep", "tp"), None))
    return jax.shard_map(body, mesh=mesh, in_specs=in_specs, out_specs=out_specs, check_vma=False)
```
